32 devices in a mesh: fs: 8 (over z, y), tp: 4 (over x, core).
Axes of the slice: x: 2, y: 2, z: 4, core: 2. Of those that a mesh axis runs over, the one named last changes fastest.
Arguments:
- tokens: bfloat16 [8192, 2048], P('fs', 'tp'), may hold values from -6 to 6
- mixer_gain: float32 [2048], replicated, may hold values from 0.1 to 1.9
- ffn_gain: float32 [2048], replicated, may hold values from 0.1 to 1.9
- w_outer: float32 [2048, 1024], P('fs', 'tp'), may hold values from -0.125 to 0.125
- w_inner: float32 [2048, 1024], P('fs', 'tp'), may hold values from -0.125 to 0.125
- w_value: float32 [2048, 1024], P('fs', 'tp'), may hold values from -0.125 to 0.125
- scale_outer: float32 [1, 1024], P(None, 'tp'), may hold values from 0.5 to 2
- scale_inner: float32 [1, 1024], P(None, 'tp'), may hold values from 0.5 to 2
- scale_value: float32 [1, 1024], P(None, 'tp'), may hold values from 0.5 to 2
- conv_taps: float32 [3, 1024], P(None, 'tp'), may hold values from -3.5 to 3.5
- w_mixout: float32 [1024, 2048], P('tp', 'fs'), may hold values from -0.1875 to 0.1875
- scale_mixout: float32 [1, 2048], P(None, 'fs'), may hold values from 0.5 to 2
- w_gate: float32 [2048, 5632], P('fs', 'tp'), may hold values from -0.125 to 0.125
- w_upward: float32 [2048, 5632], P('fs', 'tp'), may hold values from -0.125 to 0.125
- scale_gate: float32 [1, 5632], P(None, 'tp'), may hold values from 0.5 to 2
- scale_upward: float32 [1, 5632], P(None, 'tp'), may hold values from 0.5 to 2
- w_down: float32 [5632, 2048], P('tp', 'fs'), may hold values from -0.078125 to 0.078125
- scale_down: float32 [1, 2048], P(None, 'fs'), may hold values from 0.5 to 2
Outputs:
- block_out: bfloat16 [8192, 2048], P('fs', 'tp')
The draws below stay inside these ranges and needn't reach their ends.
All inputs are finite; a program needn't handle non-finite values.
Results may differ from the reference program's by a relative error of at most 0.019.
Values may be sent and summed in bfloat16 or wider, within the bound.
A program may use at most 128 MiB of HBM per device.

```python
import math
import jax
import jax.numpy as jnp
from jax import lax

MODEL = 2048
CHANNELS = 1024
HIDDEN_SIZE = 5632
TAPS = 3
SEQ_LEN = 128
TOKENS = 8192
N_TP = 4


def levels(rng, extent, pieces, low, high):
    def one(position, blocks):
        draws = jax.random.uniform(jax.random.fold_in(jax.random.fold_in(rng, 6), position), (blocks,), jnp.float32, low / len(pieces), high / len(pieces))
        return jnp.repeat(jnp.exp(draws), extent[position] // blocks).reshape((-1,) + (1,) * (len(extent) - position - 1))

    factor_of = one(*pieces[0])
    for cut in pieces[1:]:
        factor_of = factor_of * one(*cut)
    return factor_of


def scatter_about(rng, dims, deviation, reach, pieces=(), kind=jnp.bfloat16):
    result = jax.random.normal(rng, dims, jnp.float32) * deviation
    if len(pieces) > 0:
        result = levels(rng, dims, pieces, -0.22, 0.18) * result
    return jnp.clip(result, min=-reach, max=reach).astype(kind)


def setup_inputs(seed: int = 0) -> dict:
    splits = jax.random.split(jax.random.key(seed), 19)
    return {
        "tokens": scatter_about(splits[0], (TOKENS, MODEL), 1.0, 6.0, ((0, 8), (1, 4))),
        "mixer_gain": jnp.clip(1.0 + 0.18 * jax.random.normal(splits[1], (MODEL,), jnp.float32), 0.1, 1.9),
        "ffn_gain": jnp.clip(1.0 + 0.18 * jax.random.normal(splits[2], (MODEL,), jnp.float32), 0.1, 1.9),
        "w_outer": scatter_about(splits[3], (MODEL, CHANNELS), MODEL ** -0.5, 0.125, ((0, 8), (1, 4)), jnp.float32),
        "w_inner": scatter_about(splits[4], (MODEL, CHANNELS), MODEL ** -0.5, 0.125, ((0, 8), (1, 4)), jnp.float32),
        "w_value": scatter_about(splits[5], (MODEL, CHANNELS), MODEL ** -0.5, 0.125, ((0, 8), (1, 4)), jnp.float32),
        "scale_outer": jnp.clip(jnp.exp(math.log(2.0) - 1.3862944 * jax.random.uniform(splits[6], (1, CHANNELS), jnp.float32) ** levels(splits[6], (1, CHANNELS), ((1, 4),), -0.2, 0.2)), 0.5, 2.0),
        "scale_inner": jnp.clip(jnp.exp(math.log(2.0) - 1.3862944 * jax.random.uniform(splits[7], (1, CHANNELS), jnp.float32) ** levels(splits[7], (1, CHANNELS), ((1, 4),), -0.2, 0.2)), 0.5, 2.0),
        "scale_value": jnp.clip(jnp.exp(math.log(2.0) - 1.3862944 * jax.random.uniform(splits[8], (1, CHANNELS), jnp.float32) ** levels(splits[8], (1, CHANNELS), ((1, 4),), -0.2, 0.2)), 0.5, 2.0),
        "conv_taps": scatter_about(splits[9], (TAPS, CHANNELS), TAPS ** -0.5, 3.5, ((1, 4),), jnp.float32),
        "w_mixout": scatter_about(splits[10], (CHANNELS, MODEL), CHANNELS ** -0.5, 0.1875, ((0, 4), (1, 8)), jnp.float32),
        "scale_mixout": jnp.clip(jnp.exp(math.log(2.0) - 1.3862944 * jax.random.uniform(splits[11], (1, MODEL), jnp.float32) ** levels(splits[11], (1, MODEL), ((1, 8),), -0.2, 0.2)), 0.5, 2.0),
        "w_gate": scatter_about(splits[12], (MODEL, HIDDEN_SIZE), MODEL ** -0.5, 0.125, ((0, 8), (1, 4)), jnp.float32),
        "w_upward": scatter_about(splits[13], (MODEL, HIDDEN_SIZE), MODEL ** -0.5, 0.125, ((0, 8), (1, 4)), jnp.float32),
        "scale_gate": jnp.clip(jnp.exp(math.log(2.0) - 1.3862944 * jax.random.uniform(splits[14], (1, HIDDEN_SIZE), jnp.float32) ** levels(splits[14], (1, HIDDEN_SIZE), ((1, 4),), -0.2, 0.2)), 0.5, 2.0),
        "scale_upward": jnp.clip(jnp.exp(math.log(2.0) - 1.3862944 * jax.random.uniform(splits[15], (1, HIDDEN_SIZE), jnp.float32) ** levels(splits[15], (1, HIDDEN_SIZE), ((1, 4),), -0.2, 0.2)), 0.5, 2.0),
        "w_down": scatter_about(splits[16], (HIDDEN_SIZE, MODEL), HIDDEN_SIZE ** -0.5, 0.078125, ((0, 4), (1, 8)), jnp.float32),
        "scale_down": jnp.clip(jnp.exp(math.log(2.0) - 1.3862944 * jax.random.uniform(splits[17], (1, MODEL), jnp.float32) ** levels(splits[17], (1, MODEL), ((1, 8),), -0.2, 0.2)), 0.5, 2.0),
    }


def rms_scaled(full_rows, gain_vec):
    values = full_rows.astype(jnp.float32)
    inverse = lax.rsqrt(lax.optimization_barrier(jnp.mean(values * values, axis=-1, keepdims=True)) + 1e-06)
    return (values * inverse * gain_vec).astype(jnp.bfloat16)

def causal_taps(product, conv_taps):
    padded = jnp.pad(product, ((0, 0), (TAPS - 1, 0), (0, 0)))
    length = product.shape[1]
    summed = jnp.zeros(product.shape, jnp.float32)
    for tap_index in range(TAPS):
        summed = summed + conv_taps[tap_index] * padded[:, tap_index:tap_index + length, :]
    return summed

def reference(tokens, mixer_gain, ffn_gain, w_outer, w_inner, w_value, scale_outer, scale_inner, scale_value, conv_taps, w_mixout, scale_mixout, w_gate, w_upward, scale_gate, scale_upward, w_down, scale_down):
    normed = rms_scaled(tokens, mixer_gain)

    def project(weight, column_scale):
        return jnp.dot(normed, weight.astype(jnp.bfloat16), preferred_element_type=jnp.float32) * column_scale
    outer = project(w_outer, scale_outer)
    inner = project(w_inner, scale_inner)
    value = project(w_value, scale_value)
    product = (inner * value).reshape(-1, SEQ_LEN, CHANNELS)
    conv = causal_taps(product, conv_taps).reshape(-1, CHANNELS)
    mixed_out = (outer * conv).astype(jnp.bfloat16)
    mix_term = jnp.dot(mixed_out, w_mixout.astype(jnp.bfloat16), preferred_element_type=jnp.float32) * scale_mixout
    residual = (tokens.astype(jnp.float32) + mix_term).astype(jnp.bfloat16)
    normed_ffn = rms_scaled(residual, ffn_gain)
    gate_proj = jnp.dot(normed_ffn, w_gate.astype(jnp.bfloat16), preferred_element_type=jnp.float32) * scale_gate
    up_proj = jnp.dot(normed_ffn, w_upward.astype(jnp.bfloat16), preferred_element_type=jnp.float32) * scale_upward
    hidden = (jax.nn.silu(gate_proj) * up_proj).astype(jnp.bfloat16)
    down_bf = w_down.astype(jnp.bfloat16)
    block_width = HIDDEN_SIZE // N_TP

    def add_block(summed, block_index):
        offset = (block_index * block_width).astype(jnp.int32)
        left = lax.dynamic_slice_in_dim(hidden, offset, block_width, 1)
        right = lax.dynamic_slice_in_dim(down_bf, offset, block_width, 0)
        part = (jnp.dot(left, right, preferred_element_type=jnp.float32) * scale_down).astype(jnp.bfloat16)
        part = lax.optimization_barrier(part)
        return (summed + part.astype(jnp.float32), None)
    ffn_sum, _ = lax.scan(add_block, jnp.zeros(residual.shape, jnp.float32), jnp.arange(N_TP, dtype=jnp.int32))
    return (residual.astype(jnp.float32) + ffn_sum).astype(jnp.bfloat16)
```

```python
import jax
import jax.numpy as jnp
from jax import lax
from jax.experimental import pallas as pl
from jax.experimental.pallas import tpu as pltpu
from jax.sharding import PartitionSpec as P

SEQ_LEN = 128


def rms_scaled(full_rows, gain_vec):
    values = full_rows.astype(jnp.float32)
    inverse = lax.rsqrt(jnp.mean(values * values, axis=-1, keepdims=True) + 1e-06)
    return (values * inverse * gain_vec).astype(jnp.bfloat16)


def add_rows(left, w_piece):
    return jnp.dot(left, w_piece, preferred_element_type=jnp.float32)


def causal_taps(product, conv_taps):
    padded = jnp.pad(product, ((0, 0), (conv_taps.shape[0] - 1, 0), (0, 0)))
    length = product.shape[1]
    summed = jnp.zeros(product.shape, jnp.float32)
    for tap_index in range(conv_taps.shape[0]):
        summed = summed + conv_taps[tap_index] * padded[:, tap_index : tap_index + length, :]
    return summed


DEPTH, WIDTH, TP = 4, 2, 4
ROWS = 256
PIECE = 512
UP, DOWN = 0, 1
SCALES, MIXER, MIXOUT, GATED, BACK = range(5)
MESH = pl.DeviceIdType.MESH


def block_kernel(
    tokens, mixer_gain, ffn_gain, s_mixer, taps, s_gated,
    h_scales, h_mixer, h_mixout, h_gated, h_back,
    out,
    act, mixer, mixout, gated, back, scales, mixed, hidden, residual_own,
    part, from_core, from_y, from_x,
    z_send, y_send, fs_recv, tp_send, tp_recv, mx_send, mx_recv,
    act_send, act_recv, core_send, core_recv, sum_send, sum_recv, last_send, last_recv,
    local_sem,
):
    f32, bf16 = jnp.float32, jnp.bfloat16
    me, tp = lax.axis_index("fs"), lax.axis_index("tp")
    zed, why = lax.div(me, WIDTH), lax.rem(me, WIDTH)
    ex, core = lax.div(tp, 2), lax.rem(tp, 2)
    other = 1 - why
    last_z = DEPTH - 1
    count = tokens.shape[0]
    tiles = count // ROWS

    beside = zed * WIDTH + other
    sibling = ex * 2 + (1 - core)
    across = (1 - ex) * 2 + core

    barrier = pltpu.get_barrier_semaphore()
    ring = [lax.rem(zed + step, DEPTH) * WIDTH + why for step in (1, DEPTH - 1)]
    for peer in (beside, *ring):
        pl.semaphore_signal(barrier, inc=1, device_id={"fs": peer}, device_id_type=MESH)
    for peer in (sibling, across):
        pl.semaphore_signal(barrier, inc=1, device_id={"tp": peer}, device_id_type=MESH)
    pl.semaphore_wait(barrier, 5)

    fulls = (scales, mixer, mixout, gated, back)
    own_src = (h_scales, h_mixer, h_mixout, h_gated.at[why], h_back.at[why])

    def place(p, owner):
        if p in (MIXER, GATED):
            height = own_src[p].shape[0]
            return fulls[p].at[pl.ds(pl.multiple_of(owner * height, height), height), :]
        height, wide = own_src[p].shape
        first = pl.multiple_of(tp * height, height) if p == MIXOUT else 0
        return fulls[p].at[pl.ds(first, height), pl.ds(pl.multiple_of(owner * wide, wide), wide)]

    def z_copy(p, owner, way, src=None):
        spot = place(p, owner)
        step = 1 if way == UP else -1
        return pltpu.make_async_remote_copy(
            src_ref=spot if src is None else src,
            dst_ref=spot,
            send_sem=z_send.at[p, owner, way],
            recv_sem=fs_recv.at[p, owner],
            device_id={"fs": (zed + step) * WIDTH + why},
            device_id_type=MESH,
        )

    def y_copy(p, owner, src=None):
        spot = place(p, owner)
        return pltpu.make_async_remote_copy(
            src_ref=spot if src is None else src,
            dst_ref=spot,
            send_sem=y_send.at[p, owner],
            recv_sem=fs_recv.at[p, owner],
            device_id={"fs": beside},
            device_id_type=MESH,
        )

    def arrived(p, owner):
        y_copy(p, owner).wait_recv()

    def own(p):
        return pltpu.make_async_copy(own_src[p], place(p, me), local_sem.at[p])

    can_up, can_down = zed < last_z, zed > 0
    outer = (zed == 0) | (zed == last_z)

    def z_own(p, row, src):
        owner = zed * WIDTH + row
        pl.when(can_up)(lambda: z_copy(p, owner, UP, src).start())
        pl.when(can_down)(lambda: z_copy(p, owner, DOWN, src).start())

    def relay(p, s, row):
        low, high = (zed - s) * WIDTH + row, (zed + s) * WIDTH + row

        @pl.when((zed >= s) & can_up)
        def _():
            arrived(p, low)
            z_copy(p, low, UP).start()

        @pl.when((zed + s <= last_z) & can_down)
        def _():
            arrived(p, high)
            z_copy(p, high, DOWN).start()

    def settle(p, s, row):
        low, high = (zed - s) * WIDTH + row, (zed + s) * WIDTH + row
        pl.when((zed >= s) & (zed == last_z))(lambda: arrived(p, low))
        pl.when((zed + s <= last_z) & (zed == 0))(lambda: arrived(p, high))

    def mx_copy(owner, k, src=None):
        line, target = ((tp, sibling), (tp, across), (across, sibling))[k]
        height, wide = h_mixout.shape
        spot = mixout.at[
            pl.ds(pl.multiple_of(line * height, height), height),
            pl.ds(pl.multiple_of(owner * wide, wide), wide),
        ]
        return pltpu.make_async_remote_copy(
            src_ref=spot if src is None else src,
            dst_ref=spot,
            send_sem=mx_send.at[owner, k],
            recv_sem=mx_recv.at[owner, k],
            device_id={"tp": target},
            device_id_type=MESH,
        )

    def mx_first(owner, src=None):
        mx_copy(owner, 1, src).start()
        mx_copy(owner, 0, src).start()

    firsts = (SCALES, MIXOUT, MIXER)

    def relay_first(s):
        low, high = (zed - s) * WIDTH + why, (zed + s) * WIDTH + why

        @pl.when(zed >= s)
        def _():
            for p in firsts:
                arrived(p, low)
                pl.when(can_up)(lambda: z_copy(p, low, UP).start())
                y_copy(p, low).start()
                if p == MIXOUT:
                    mx_first(low)

        @pl.when(zed + s <= last_z)
        def _():
            for p in firsts:
                arrived(p, high)
                pl.when(can_down)(lambda: z_copy(p, high, DOWN).start())
                y_copy(p, high).start()
                if p == MIXOUT:
                    mx_first(high)

    def from_beside(s):
        def take(owner):
            for p in firsts:
                arrived(p, owner)
                if p == MIXOUT:
                    mx_first(owner)

        if s == 0:
            take(beside)
            return
        low, high = (zed - s) * WIDTH + other, (zed + s) * WIDTH + other
        pl.when(zed >= s)(lambda: take(low))
        pl.when(zed + s <= last_z)(lambda: take(high))

    base = pl.multiple_of(why * count, count)

    def tp_slot(a, owner):
        if a == 0:
            wide = tokens.shape[1]
            return act.at[pl.ds(base, count), pl.ds(pl.multiple_of(owner * wide, wide), wide)]
        wide = mixed.shape[1] // TP
        return mixed.at[:, pl.ds(pl.multiple_of(owner * wide, wide), wide)]

    def tp_copy(a, k):
        owner, target = ((tp, sibling), (tp, across), (across, sibling))[k]
        spot = tp_slot(a, owner)
        return pltpu.make_async_remote_copy(
            src_ref=tokens if a == 0 and k < 2 else spot,
            dst_ref=spot,
            send_sem=tp_send.at[a, k],
            recv_sem=tp_recv.at[a, k],
            device_id={"tp": target},
            device_id_type=MESH,
        )

    def tp_first(a):
        tp_copy(a, 1).start()
        tp_copy(a, 0).start()

    def tp_second(a):
        tp_copy(a, 1).wait_recv()
        tp_copy(a, 2).start()

    def tp_finish(a):
        tp_copy(a, 0).wait_recv()
        tp_copy(a, 2).wait_recv()

    own_tokens = pltpu.make_async_copy(tokens, tp_slot(0, tp), local_sem.at[5])

    for p in firsts:
        y_copy(p, me, own_src[p]).start()
        z_own(p, why, own_src[p])
    tp_first(0)
    mx_first(me, h_mixout)
    own_tokens.start()
    for p in range(5):
        own(p).start()
    units = h_back.shape[1]
    back[units:, :] = jnp.zeros((back.shape[0] - units, back.shape[1]), bf16)

    relay_first(1)
    tp_second(0)
    relay_first(2)
    z_own(GATED, why, own_src[GATED])
    relay_first(3)
    for p in (GATED, BACK):
        y_copy(p, me, (h_gated if p == GATED else h_back).at[other]).start()
    for s in range(DEPTH):
        from_beside(s)
    relay(GATED, 1, why)
    tp_finish(0)
    own_tokens.wait()
    for p in firsts:
        own(p).wait()

    chan = mixed.shape[1] // TP

    def tile(i):
        return pl.ds(pl.multiple_of(i * ROWS, ROWS), ROWS)

    def own_rows(i):
        return pl.ds(pl.multiple_of(base + i * ROWS, ROWS), ROWS)

    def normalised(values, gain):
        inverse = lax.rsqrt(jnp.mean(values * values, axis=-1, keepdims=True) + 1e-06)
        return (values * inverse * gain[...]).astype(bf16)

    @pl.loop(0, tiles)
    def _(i):
        normed = normalised(act[own_rows(i), :].astype(f32), mixer_gain)
        three = jnp.dot(normed, mixer[...], preferred_element_type=f32) * s_mixer[...]
        product = three[:, chan : 2 * chan] * three[:, 2 * chan :]
        row = lax.rem(lax.broadcasted_iota(jnp.int32, product.shape, 0), SEQ_LEN)
        total = jnp.zeros_like(product)
        last = taps.shape[0] - 1
        for j in range(taps.shape[0]):
            gap = last - j
            moved = product
            if gap:
                moved = jnp.where(row >= gap, pltpu.roll(product, gap, 0), 0.0)
            total = total + taps[j : j + 1, :] * moved
        mixed[tile(i), pl.ds(pl.multiple_of(tp * chan, chan), chan)] = (
            three[:, :chan] * total
        ).astype(bf16)

    tp_first(1)
    relay(GATED, 2, why)
    arrived(GATED, beside)
    z_own(GATED, other, None)
    for owner in range(DEPTH * WIDTH):
        mx_copy(owner, 1).wait_recv()
        mx_copy(owner, 2).start()
    tp_second(1)
    relay(GATED, 1, other)
    for owner in range(DEPTH * WIDTH):
        mx_copy(owner, 0).wait_recv()
        mx_copy(owner, 2).wait_recv()
    tp_finish(1)
    for k in range(3):
        tp_copy(0, k).wait_send()

    feat = tokens.shape[1]
    share = tiles // 2

    def act_copy(half, lead, q, k):
        spot = act.at[
            pl.ds(pl.multiple_of(half * count + (lead * share + q) * ROWS, ROWS), ROWS), :
        ]
        return pltpu.make_async_remote_copy(
            src_ref=spot,
            dst_ref=spot,
            send_sem=act_send.at[q, k],
            recv_sem=act_recv.at[q, k],
            device_id={"fs": beside} if k == 0 else {"tp": sibling},
            device_id_type=MESH,
        )

    @pl.loop(0, tiles)
    def _(step):
        i = lax.rem(step + core * share, tiles)
        term = jnp.dot(mixed[tile(i), :], mixout[...], preferred_element_type=f32)
        term = term * scales[0:1, :]
        residual = (act[own_rows(i), :].astype(f32) + term).astype(bf16)
        act[own_rows(i), :] = residual
        residual_own[tile(i), :] = act[
            own_rows(i), pl.ds(pl.multiple_of(tp * feat, feat), feat)
        ]
        act[own_rows(i), :] = normalised(residual.astype(f32), ffn_gain)
        pl.when(step < share)(lambda: act_copy(why, core, step, 0).start())

    z_own(BACK, why, own_src[BACK])
    arrived(BACK, beside)
    z_own(BACK, other, None)
    relay(GATED, 2, other)
    for row in (why, other):
        for s in (1, 2):
            relay(BACK, s, row)
    for q in range(share):
        act_copy(other, core, q, 0).wait_recv()
        act_copy(other, core, q, 1).start()
    own(GATED).wait()
    for row in (why, other):
        for s in (1, 2, 3):
            settle(GATED, s, row)

    main = (gated.shape[1] // 256) * 128

    def activate(first, steps):
        @pl.loop(0, steps)
        def _(i):
            rows = pl.ds(pl.multiple_of(first + i * ROWS, ROWS), ROWS)
            both = jnp.dot(act[rows, :], gated[...], preferred_element_type=f32)
            both = both * s_gated[pl.ds(why, 1), :]
            gate, up = both[:, :main], both[:, main + 128 :]
            hidden[rows, :main] = (gate / (1.0 + jnp.exp(-gate)) * up).astype(bf16)
            gate = both[:, main : main + 128]
            up = pltpu.roll(gate, 64, 1)
            rest = gate / (1.0 + jnp.exp(-gate)) * up
            lane = lax.broadcasted_iota(jnp.int32, rest.shape, 1)
            hidden[rows, main:] = jnp.where(lane < 64, rest, 0.0).astype(bf16)

    activate(base, tiles)
    for q in range(share):
        act_copy(other, 1 - core, q, 1).wait_recv()
    activate(other * count, tiles)

    own(BACK).wait()
    pieces = count // PIECE

    def piece(t):
        return pl.ds(pl.multiple_of(t * PIECE, PIECE), PIECE)

    def block_at(k):
        return lax.rem(zed + k * (1 - 2 * lax.div(zed, last_z)) + DEPTH, DEPTH)

    def core_copy(j, t):
        line = lax.div(j, 2)
        return pltpu.make_async_remote_copy(
            src_ref=part.at[j, piece(t), :],
            dst_ref=from_core.at[line, piece(t), :],
            send_sem=core_send.at[line, t],
            recv_sem=core_recv.at[line, t],
            device_id={"tp": sibling},
            device_id_type=MESH,
        )

    def sum_copy(j, q):
        line = lax.div(j, 2)
        return pltpu.make_async_remote_copy(
            src_ref=part.at[j, piece(other * pieces + q), :],
            dst_ref=from_y.at[line, piece(q), :],
            send_sem=sum_send.at[line, q],
            recv_sem=sum_recv.at[line, q],
            device_id={"fs": beside},
            device_id_type=MESH,
        )

    def last_copy(j, q):
        return pltpu.make_async_remote_copy(
            src_ref=part.at[j, piece(why * pieces + q), :],
            dst_ref=from_x.at[piece(q), :],
            send_sem=last_send.at[q],
            recv_sem=last_recv.at[q],
            device_id={"tp": across},
            device_id_type=MESH,
        )

    def multiply(k):
        j = block_at(k)
        if k:
            for row in range(WIDTH):
                pl.when(outer)(lambda: arrived(BACK, j * WIDTH + row))
        columns = pl.ds(pl.multiple_of(j * feat, feat), feat)

        @pl.loop(0, WIDTH * pieces)
        def _(step):
            t = lax.rem(step + other * pieces, WIDTH * pieces)
            term = jnp.dot(hidden[piece(t), :], back[:, columns], preferred_element_type=f32)
            part[j, piece(t), :] = (term * scales[8:9, columns]).astype(bf16)
            pl.when(core != lax.rem(j, 2))(lambda: core_copy(j, t).start())

    def added(j, t, extra):
        return part[j, piece(t), :].astype(f32) + extra.astype(f32)

    def reduce_core(k):
        j = block_at(k)

        @pl.when(core == lax.rem(j, 2))
        def _():
            line = lax.div(j, 2)
            for half in (other, why):
                for q in range(pieces):
                    t = half * pieces + q
                    core_copy(j, t).wait_recv()
                    part[j, piece(t), :] = added(j, t, from_core[line, piece(t), :]).astype(bf16)
                    if half is other:
                        sum_copy(j, q).start()

    def reduce_y(k):
        j = block_at(k)

        @pl.when(core == lax.rem(j, 2))
        def _():
            line = lax.div(j, 2)
            for q in range(pieces):
                t = why * pieces + q
                sum_copy(j, q).wait_recv()
                part[j, piece(t), :] = added(j, t, from_y[line, piece(q), :]).astype(bf16)
                pl.when(ex != line)(lambda: last_copy(j, q).start())

    def reduce_x(k):
        j = block_at(k)

        @pl.when(tp == j)
        def _():
            for q in range(pieces):
                t = why * pieces + q
                last_copy(j, q).wait_recv()
                total = added(j, t, from_x[piece(q), :])
                out[piece(q), :] = (residual_own[piece(q), :].astype(f32) + total).astype(bf16)

    for k in range(DEPTH):
        multiply(k)
        reduce_core(k)
        if k > 0:
            reduce_y(k - 1)
        if k > 1:
            reduce_x(k - 2)
    reduce_y(DEPTH - 1)
    reduce_x(DEPTH - 2)
    reduce_x(DEPTH - 1)

    def sent(p, row):
        owner = zed * WIDTH + row
        pl.when(can_up)(lambda: z_copy(p, owner, UP).wait_send())
        pl.when(can_down)(lambda: z_copy(p, owner, DOWN).wait_send())
        for s in (1, 2):
            low, high = (zed - s) * WIDTH + row, (zed + s) * WIDTH + row
            pl.when((zed >= s) & can_up)(lambda: z_copy(p, low, UP).wait_send())
            pl.when((zed + s <= last_z) & can_down)(lambda: z_copy(p, high, DOWN).wait_send())

    for p in range(5):
        sent(p, why)
        y_copy(p, me).wait_send()
        if p in (GATED, BACK):
            sent(p, other)
        else:
            for s in (1, 2, 3):
                low, high = (zed - s) * WIDTH + why, (zed + s) * WIDTH + why
                pl.when(zed >= s)(lambda: y_copy(p, low).wait_send())
                pl.when(zed + s <= last_z)(lambda: y_copy(p, high).wait_send())
    for owner in range(DEPTH * WIDTH):
        for k in range(3):
            mx_copy(owner, k).wait_send()
    for k in range(3):
        tp_copy(1, k).wait_send()
    for q in range(share):
        act_copy(why, core, q, 0).wait_send()
        act_copy(other, core, q, 1).wait_send()
    for j in range(DEPTH):

        @pl.when(core != j % 2)
        def _():
            for t in range(WIDTH * pieces):
                core_copy(j, t).wait_send()

        @pl.when(core == j % 2)
        def _():
            for q in range(pieces):
                sum_copy(j, q).wait_send()
                pl.when(ex != j // 2)(lambda: last_copy(j, q).wait_send())


def halves(gate, up, axis_units):
    half = axis_units // 2
    main = half // 128 * 128
    end = axis_units - main
    return jnp.stack(
        [
            jnp.concatenate(
                [gate[:, :main], gate[:, main:half], up[:, main:half], up[:, :main]], axis=1
            ),
            jnp.concatenate(
                [gate[:, end:], gate[:, half:end], up[:, half:end], up[:, end:]], axis=1
            ),
        ]
    )


def fused_device(
    tokens,
    mixer_gain,
    ffn_gain,
    w_outer,
    w_inner,
    w_value,
    scale_outer,
    scale_inner,
    scale_value,
    conv_taps,
    w_mixout,
    scale_mixout,
    w_gate,
    w_upward,
    scale_gate,
    scale_upward,
    w_down,
    scale_down,
):
    bf16 = jnp.bfloat16
    count, feat = tokens.shape
    model = mixer_gain.shape[0]
    chan = w_outer.shape[1]
    units = w_gate.shape[1]
    cols = w_down.shape[1]
    half = units // 2
    main = half // 128 * 128
    padded = main + 128
    shard = jnp.concatenate([w_outer, w_inner, w_value], axis=1).astype(bf16)
    s_mixer = jnp.concatenate([scale_outer, scale_inner, scale_value], axis=1)
    scale_shard = jnp.concatenate(
        [jnp.broadcast_to(scale_mixout, (8, cols)), jnp.broadcast_to(scale_down, (8, cols))], axis=0
    )
    h_gated = halves(w_gate.astype(bf16), w_upward.astype(bf16), units)
    s_gated = halves(scale_gate, scale_upward, units)[:, 0]
    w_back = w_down.astype(bf16)
    h_back = jnp.stack(
        [w_back[:half], jnp.concatenate([w_back[units - main :], w_back[half : units - main]])]
    )
    vmem = pl.BlockSpec(memory_space=pltpu.VMEM)
    dma = pltpu.SemaphoreType.DMA
    owners = DEPTH * WIDTH
    return pl.pallas_call(
        block_kernel,
        out_shape=jax.ShapeDtypeStruct((count, feat), bf16),
        in_specs=[vmem] * 11,
        out_specs=vmem,
        scratch_shapes=[
            pltpu.VMEM((WIDTH * count, model), bf16),
            pltpu.VMEM((model, 3 * chan), bf16),
            pltpu.VMEM((TP * chan, model), bf16),
            pltpu.VMEM((model, units), bf16),
            pltpu.VMEM((padded, model), bf16),
            pltpu.VMEM((16, model), jnp.float32),
            pltpu.VMEM((count, TP * chan), bf16),
            pltpu.VMEM((WIDTH * count, padded), bf16),
            pltpu.VMEM((count, feat), bf16),
            pltpu.VMEM((DEPTH, WIDTH * count, feat), bf16),
            pltpu.VMEM((2, WIDTH * count, feat), bf16),
            pltpu.VMEM((2, count, feat), bf16),
            pltpu.VMEM((count, feat), bf16),
            dma((5, owners, 2)),
            dma((5, owners)),
            dma((5, owners)),
            dma((2, 3)),
            dma((2, 3)),
            dma((owners, 3)),
            dma((owners, 3)),
            dma((2, 2)),
            dma((2, 2)),
            dma((2, 4)),
            dma((2, 4)),
            dma((2, 2)),
            dma((2, 2)),
            dma((2,)),
            dma((2,)),
            dma((6,)),
        ],
        compiler_params=pltpu.CompilerParams(
            collective_id=0, has_side_effects=True, vmem_limit_bytes=62 * 1024 * 1024
        ),
    )(
        tokens, mixer_gain[None], ffn_gain[None], s_mixer, conv_taps, s_gated,
        scale_shard, shard, w_mixout.astype(bf16), h_gated, h_back,
    )


def plain_device(
    tokens,
    mixer_gain,
    ffn_gain,
    w_outer,
    w_inner,
    w_value,
    scale_outer,
    scale_inner,
    scale_value,
    conv_taps,
    w_mixout,
    scale_mixout,
    w_gate,
    w_upward,
    scale_gate,
    scale_upward,
    w_down,
    scale_down,
):
    full_rows = lax.all_gather(tokens, "tp", axis=1, tiled=True)
    normed = rms_scaled(full_rows, mixer_gain)
    tok_count = tokens.shape[0]
    local_channels = w_outer.shape[1]

    def add_one(w_piece):
        return add_rows(normed, w_piece)

    outer_bf = w_outer.astype(jnp.bfloat16)
    inner_bf = w_inner.astype(jnp.bfloat16)
    value_bf = w_value.astype(jnp.bfloat16)
    outer = add_one(lax.all_gather(outer_bf, "fs", axis=0, tiled=True))
    inner = add_one(lax.all_gather(inner_bf, "fs", axis=0, tiled=True))
    value = add_one(lax.all_gather(value_bf, "fs", axis=0, tiled=True))
    outer = outer * scale_outer
    product = inner * scale_inner * (value * scale_value)
    product = product.reshape(tok_count // SEQ_LEN, SEQ_LEN, local_channels)
    conv = causal_taps(product, conv_taps).reshape(tok_count, local_channels)
    mixed_out = (outer * conv).astype(jnp.bfloat16)
    mixout_scales, down_scales = (
        lax.all_gather(scale_mixout, "fs", axis=1, tiled=True),
        lax.all_gather(scale_down, "fs", axis=1, tiled=True),
    )
    mixout_bf = w_mixout.astype(jnp.bfloat16)
    mixed_all = lax.all_gather(mixed_out, "tp", axis=1, tiled=True)
    mixout_cols = lax.all_gather(mixout_bf, "fs", axis=1, tiled=True)
    mixout_all = lax.all_gather(mixout_cols, "tp", axis=0, tiled=True)
    mix_term = jnp.dot(mixed_all, mixout_all, preferred_element_type=jnp.float32) * mixout_scales
    residual_rows = (full_rows.astype(jnp.float32) + mix_term).astype(jnp.bfloat16)
    feature_count = tokens.shape[1]
    residual = lax.dynamic_slice_in_dim(
        residual_rows, lax.axis_index("tp") * feature_count, feature_count, 1
    )
    normed_ffn = rms_scaled(residual_rows, ffn_gain)
    gate_proj = add_rows(
        normed_ffn, lax.all_gather(w_gate.astype(jnp.bfloat16), "fs", axis=0, tiled=True)
    )
    up_proj = add_rows(
        normed_ffn, lax.all_gather(w_upward.astype(jnp.bfloat16), "fs", axis=0, tiled=True)
    )
    hidden = (jax.nn.silu(gate_proj * scale_gate) * (up_proj * scale_upward)).astype(jnp.bfloat16)
    down_terms = (
        jnp.dot(
            hidden,
            lax.all_gather(w_down.astype(jnp.bfloat16), "fs", axis=1, tiled=True),
            preferred_element_type=jnp.float32,
        )
        * down_scales
    )
    ffn_share = lax.psum_scatter(
        down_terms.astype(jnp.bfloat16), "tp", scatter_dimension=1, tiled=True
    ).astype(jnp.float32)
    return (residual.astype(jnp.float32) + ffn_share).astype(jnp.bfloat16)


def solution(mesh):
    in_specs = (
        P("fs", "tp"),
        P(),
        P(),
        P("fs", "tp"),
        P("fs", "tp"),
        P("fs", "tp"),
        P(None, "tp"),
        P(None, "tp"),
        P(None, "tp"),
        P(None, "tp"),
        P("tp", "fs"),
        P(None, "fs"),
        P("fs", "tp"),
        P("fs", "tp"),
        P(None, "tp"),
        P(None, "tp"),
        P("tp", "fs"),
        P(None, "fs"),
    )
    out_specs = P("fs", "tp")
    chosen = fused_device if (mesh.shape["fs"], mesh.shape["tp"]) == (8, 4) else plain_device
    return jax.shard_map(
        chosen, mesh=mesh, in_specs=in_specs, out_specs=out_specs, check_vma=False
    )
```

```python
import jax
import jax.numpy as jnp
from jax import lax
from jax.experimental import pallas as pl
from jax.experimental.pallas import tpu as pltpu
from jax.sharding import PartitionSpec as P

SEQ_LEN = 128


def rms_scaled(full_rows, gain_vec):
    values = full_rows.astype(jnp.float32)
    inverse = lax.rsqrt(jnp.mean(values * values, axis=-1, keepdims=True) + 1e-06)
    return (values * inverse * gain_vec).astype(jnp.bfloat16)


def add_rows(left, w_piece):
    return jnp.dot(left, w_piece, preferred_element_type=jnp.float32)


def causal_taps(product, conv_taps):
    padded = jnp.pad(product, ((0, 0), (conv_taps.shape[0] - 1, 0), (0, 0)))
    length = product.shape[1]
    summed = jnp.zeros(product.shape, jnp.float32)
    for tap_index in range(conv_taps.shape[0]):
        summed = summed + conv_taps[tap_index] * padded[:, tap_index : tap_index + length, :]
    return summed


DEPTH, WIDTH, TP = 4, 2, 4
ROWS = 256
PIECE = 512
UP, DOWN = 0, 1
SCALES, MIXER, MIXOUT, GATED, BACK = range(5)
MESH = pl.DeviceIdType.MESH


def block_kernel(
    tokens, mixer_gain, ffn_gain, w_outer, w_inner, w_value, s_outer, s_inner, s_value, taps,
    w_mixout, s_mixout, w_gate, w_upward, s_gate, s_upward, w_down, s_down,
    out,
    h_scales, h_mixer, h_mixout, h_gated, h_back, s_gated, raw_gate, raw_up, raw_down,
    act, mixer, mixout, gated, back, scales, mixed, hidden, residual_own,
    part, from_core, from_y, from_x,
    z_send, y_send, fs_recv, tp_send, tp_recv, mx_send, mx_recv,
    act_send, act_recv, core_send, core_recv, sum_send, sum_recv, last_send, last_recv,
    local_sem,
):
    f32, bf16 = jnp.float32, jnp.bfloat16
    me, tp = lax.axis_index("fs"), lax.axis_index("tp")
    zed, why = lax.div(me, WIDTH), lax.rem(me, WIDTH)
    ex, core = lax.div(tp, 2), lax.rem(tp, 2)
    other = 1 - why
    last_z = DEPTH - 1
    count = tokens.shape[0]
    tiles = count // ROWS

    beside = zed * WIDTH + other
    sibling = ex * 2 + (1 - core)
    across = (1 - ex) * 2 + core

    def fetch(k):
        source, target = ((w_gate, raw_gate), (w_upward, raw_up), (w_down, raw_down))[k]
        return pltpu.make_async_copy(source, target, local_sem.at[6 + k])

    for k in range(3):
        fetch(k).start()
    barrier = pltpu.get_barrier_semaphore()
    ring = [lax.rem(zed + step, DEPTH) * WIDTH + why for step in (1, DEPTH - 1)]
    for peer in (beside, *ring):
        pl.semaphore_signal(barrier, inc=1, device_id={"fs": peer}, device_id_type=MESH)
    for peer in (sibling, across):
        pl.semaphore_signal(barrier, inc=1, device_id={"tp": peer}, device_id_type=MESH)
    wide = w_outer.shape[1]
    for k, w in enumerate((w_outer, w_inner, w_value)):
        h_mixer[:, k * wide : (k + 1) * wide] = w[...].astype(bf16)
    h_mixout[...] = w_mixout[...].astype(bf16)
    for k, row in enumerate((s_mixout, s_down)):
        h_scales[k * 8 : (k + 1) * 8, :] = jnp.broadcast_to(row[...], (8, row.shape[1]))
    pl.semaphore_wait(barrier, 5)

    fulls = (scales, mixer, mixout, gated, back)
    own_src = (h_scales, h_mixer, h_mixout, h_gated.at[why], h_back.at[why])

    def place(p, owner):
        if p in (MIXER, GATED):
            height = own_src[p].shape[0]
            return fulls[p].at[pl.ds(pl.multiple_of(owner * height, height), height), :]
        height, wide = own_src[p].shape
        first = pl.multiple_of(tp * height, height) if p == MIXOUT else 0
        return fulls[p].at[pl.ds(first, height), pl.ds(pl.multiple_of(owner * wide, wide), wide)]

    def z_copy(p, owner, way, src=None):
        spot = place(p, owner)
        step = 1 if way == UP else -1
        return pltpu.make_async_remote_copy(
            src_ref=spot if src is None else src,
            dst_ref=spot,
            send_sem=z_send.at[p, owner, way],
            recv_sem=fs_recv.at[p, owner],
            device_id={"fs": (zed + step) * WIDTH + why},
            device_id_type=MESH,
        )

    def y_copy(p, owner, src=None):
        spot = place(p, owner)
        return pltpu.make_async_remote_copy(
            src_ref=spot if src is None else src,
            dst_ref=spot,
            send_sem=y_send.at[p, owner],
            recv_sem=fs_recv.at[p, owner],
            device_id={"fs": beside},
            device_id_type=MESH,
        )

    def arrived(p, owner):
        y_copy(p, owner).wait_recv()

    def own(p):
        return pltpu.make_async_copy(own_src[p], place(p, me), local_sem.at[p])

    can_up, can_down = zed < last_z, zed > 0
    outer = (zed == 0) | (zed == last_z)

    def z_own(p, row, src):
        owner = zed * WIDTH + row
        pl.when(can_up)(lambda: z_copy(p, owner, UP, src).start())
        pl.when(can_down)(lambda: z_copy(p, owner, DOWN, src).start())

    def relay(p, s, row):
        low, high = (zed - s) * WIDTH + row, (zed + s) * WIDTH + row

        @pl.when((zed >= s) & can_up)
        def _():
            arrived(p, low)
            z_copy(p, low, UP).start()

        @pl.when((zed + s <= last_z) & can_down)
        def _():
            arrived(p, high)
            z_copy(p, high, DOWN).start()

    def settle(p, s, row):
        low, high = (zed - s) * WIDTH + row, (zed + s) * WIDTH + row
        pl.when((zed >= s) & (zed == last_z))(lambda: arrived(p, low))
        pl.when((zed + s <= last_z) & (zed == 0))(lambda: arrived(p, high))

    def mx_copy(owner, k, src=None):
        line, target = ((tp, sibling), (tp, across), (across, sibling))[k]
        height, wide = h_mixout.shape
        spot = mixout.at[
            pl.ds(pl.multiple_of(line * height, height), height),
            pl.ds(pl.multiple_of(owner * wide, wide), wide),
        ]
        return pltpu.make_async_remote_copy(
            src_ref=spot if src is None else src,
            dst_ref=spot,
            send_sem=mx_send.at[owner, k],
            recv_sem=mx_recv.at[owner, k],
            device_id={"tp": target},
            device_id_type=MESH,
        )

    def mx_first(owner, src=None):
        mx_copy(owner, 1, src).start()
        mx_copy(owner, 0, src).start()

    firsts = (SCALES, MIXOUT, MIXER)

    def relay_first(s):
        low, high = (zed - s) * WIDTH + why, (zed + s) * WIDTH + why

        @pl.when(zed >= s)
        def _():
            for p in firsts:
                arrived(p, low)
                pl.when(can_up)(lambda: z_copy(p, low, UP).start())
                y_copy(p, low).start()
                if p == MIXOUT:
                    mx_first(low)

        @pl.when(zed + s <= last_z)
        def _():
            for p in firsts:
                arrived(p, high)
                pl.when(can_down)(lambda: z_copy(p, high, DOWN).start())
                y_copy(p, high).start()
                if p == MIXOUT:
                    mx_first(high)

    def from_beside(s):
        def take(owner):
            for p in firsts:
                arrived(p, owner)
                if p == MIXOUT:
                    mx_first(owner)

        if s == 0:
            take(beside)
            return
        low, high = (zed - s) * WIDTH + other, (zed + s) * WIDTH + other
        pl.when(zed >= s)(lambda: take(low))
        pl.when(zed + s <= last_z)(lambda: take(high))

    base = pl.multiple_of(why * count, count)

    def tp_slot(a, owner):
        if a == 0:
            wide = tokens.shape[1]
            return act.at[pl.ds(base, count), pl.ds(pl.multiple_of(owner * wide, wide), wide)]
        wide = mixed.shape[1] // TP
        return mixed.at[:, pl.ds(pl.multiple_of(owner * wide, wide), wide)]

    def tp_copy(a, k):
        owner, target = ((tp, sibling), (tp, across), (across, sibling))[k]
        spot = tp_slot(a, owner)
        return pltpu.make_async_remote_copy(
            src_ref=tokens if a == 0 and k < 2 else spot,
            dst_ref=spot,
            send_sem=tp_send.at[a, k],
            recv_sem=tp_recv.at[a, k],
            device_id={"tp": target},
            device_id_type=MESH,
        )

    def tp_first(a):
        tp_copy(a, 1).start()
        tp_copy(a, 0).start()

    def tp_second(a):
        tp_copy(a, 1).wait_recv()
        tp_copy(a, 2).start()

    def tp_finish(a):
        tp_copy(a, 0).wait_recv()
        tp_copy(a, 2).wait_recv()

    own_tokens = pltpu.make_async_copy(tokens, tp_slot(0, tp), local_sem.at[5])

    for p in firsts:
        y_copy(p, me, own_src[p]).start()
        z_own(p, why, own_src[p])
    tp_first(0)
    mx_first(me, h_mixout)
    own_tokens.start()
    for p in firsts:
        own(p).start()
    units = h_back.shape[1]
    main = units // 128 * 128
    middle, after = pl.ds(main, 128), main + 128

    def share_out(gate, up, write):
        write(0, pl.ds(0, main), gate[:, :main])
        write(0, pl.ds(after, main), up[:, :main])
        write(1, pl.ds(0, main), gate[:, after:])
        write(1, pl.ds(after, main), up[:, after:])
        gate, up = gate[:, middle], up[:, middle]
        low = lax.broadcasted_iota(jnp.int32, gate.shape, 1) < 64
        write(0, middle, jnp.where(low, gate, pltpu.roll(up, 64, 1)))
        write(1, middle, jnp.where(low, pltpu.roll(gate, 64, 1), up))

    def write_scale(half, lanes, values):
        s_gated[half : half + 1, lanes] = values

    def write_gated(half, lanes, values):
        h_gated[half, :, lanes] = values.astype(bf16)

    for k in range(3):
        fetch(k).wait()
    share_out(raw_gate, raw_up, write_gated)
    h_back[0] = raw_down[:units, :].astype(bf16)
    h_back[1, :main, :] = raw_down[after:, :].astype(bf16)
    h_back[1, main:, :] = raw_down[units:after, :].astype(bf16)
    spread = [jnp.broadcast_to(row[...], (8, row.shape[1])) for row in (s_gate, s_upward)]
    share_out(
        *spread, lambda half, lanes, values: write_scale(half, lanes, values[0:1])
    )
    for p in (GATED, BACK):
        own(p).start()
    back[units:, :] = jnp.zeros((back.shape[0] - units, back.shape[1]), bf16)

    relay_first(1)
    tp_second(0)
    relay_first(2)
    z_own(GATED, why, own_src[GATED])
    relay_first(3)
    for p in (GATED, BACK):
        y_copy(p, me, (h_gated if p == GATED else h_back).at[other]).start()
    for s in range(DEPTH):
        from_beside(s)
    relay(GATED, 1, why)
    tp_finish(0)
    own_tokens.wait()
    for p in firsts:
        own(p).wait()

    chan = mixed.shape[1] // TP

    def tile(i):
        return pl.ds(pl.multiple_of(i * ROWS, ROWS), ROWS)

    def own_rows(i):
        return pl.ds(pl.multiple_of(base + i * ROWS, ROWS), ROWS)

    def normalised(values, gain):
        inverse = lax.rsqrt(jnp.mean(values * values, axis=-1, keepdims=True) + 1e-06)
        return (values * inverse * gain[...]).astype(bf16)

    @pl.loop(0, tiles)
    def _(i):
        normed = normalised(act[own_rows(i), :].astype(f32), mixer_gain)
        three = jnp.dot(normed, mixer[...], preferred_element_type=f32)
        product = (three[:, chan : 2 * chan] * s_inner[...]) * (three[:, 2 * chan :] * s_value[...])
        row = lax.rem(lax.broadcasted_iota(jnp.int32, product.shape, 0), SEQ_LEN)
        total = jnp.zeros_like(product)
        last = taps.shape[0] - 1
        for j in range(taps.shape[0]):
            gap = last - j
            moved = product
            if gap:
                moved = jnp.where(row >= gap, pltpu.roll(product, gap, 0), 0.0)
            total = total + taps[j : j + 1, :] * moved
        mixed[tile(i), pl.ds(pl.multiple_of(tp * chan, chan), chan)] = (
            three[:, :chan] * s_outer[...] * total
        ).astype(bf16)

    tp_first(1)
    relay(GATED, 2, why)
    arrived(GATED, beside)
    z_own(GATED, other, None)
    for owner in range(DEPTH * WIDTH):
        mx_copy(owner, 1).wait_recv()
        mx_copy(owner, 2).start()
    tp_second(1)
    relay(GATED, 1, other)
    for owner in range(DEPTH * WIDTH):
        mx_copy(owner, 0).wait_recv()
        mx_copy(owner, 2).wait_recv()
    tp_finish(1)
    for k in range(3):
        tp_copy(0, k).wait_send()

    feat = tokens.shape[1]
    share = tiles // 2

    def act_copy(half, lead, q, k):
        spot = act.at[
            pl.ds(pl.multiple_of(half * count + (lead * share + q) * ROWS, ROWS), ROWS), :
        ]
        return pltpu.make_async_remote_copy(
            src_ref=spot,
            dst_ref=spot,
            send_sem=act_send.at[q, k],
            recv_sem=act_recv.at[q, k],
            device_id={"fs": beside} if k == 0 else {"tp": sibling},
            device_id_type=MESH,
        )

    @pl.loop(0, tiles)
    def _(step):
        i = lax.rem(step + core * share, tiles)
        term = jnp.dot(mixed[tile(i), :], mixout[...], preferred_element_type=f32)
        term = term * scales[0:1, :]
        residual = (act[own_rows(i), :].astype(f32) + term).astype(bf16)
        act[own_rows(i), :] = residual
        residual_own[tile(i), :] = act[
            own_rows(i), pl.ds(pl.multiple_of(tp * feat, feat), feat)
        ]
        act[own_rows(i), :] = normalised(residual.astype(f32), ffn_gain)
        pl.when(step < share)(lambda: act_copy(why, core, step, 0).start())

    relay(GATED, 2, other)
    arrived(BACK, beside)
    own(BACK).wait()
    for row in range(WIDTH):
        z_own(BACK, row, None)
    for q in range(share):
        act_copy(other, core, q, 0).wait_recv()
        act_copy(other, core, q, 1).start()
    own(GATED).wait()
    for row in (why, other):
        for s in (1, 2, 3):
            settle(GATED, s, row)

    def activate(first, steps):
        @pl.loop(0, steps)
        def _(i):
            rows = pl.ds(pl.multiple_of(first + i * ROWS, ROWS), ROWS)
            both = jnp.dot(act[rows, :], gated[...], preferred_element_type=f32)
            both = both * s_gated[pl.ds(why, 1), :]
            gate, up = both[:, :main], both[:, main + 128 :]
            hidden[rows, :main] = (gate / (1.0 + jnp.exp(-gate)) * up).astype(bf16)
            gate = both[:, main : main + 128]
            up = pltpu.roll(gate, 64, 1)
            rest = gate / (1.0 + jnp.exp(-gate)) * up
            lane = lax.broadcasted_iota(jnp.int32, rest.shape, 1)
            hidden[rows, main:] = jnp.where(lane < 64, rest, 0.0).astype(bf16)

    pieces = count // PIECE

    def piece(t):
        return pl.ds(pl.multiple_of(t * PIECE, PIECE), PIECE)

    def block_at(k):
        return lax.rem(zed + k * (1 - 2 * lax.div(zed, last_z)) + DEPTH, DEPTH)

    def core_copy(j, row, t):
        line = lax.div(j, 2)
        return pltpu.make_async_remote_copy(
            src_ref=part.at[j, row, piece(t), :],
            dst_ref=from_core.at[line, row, piece(t), :],
            send_sem=core_send.at[line, row, t],
            recv_sem=core_recv.at[line, row, t],
            device_id={"tp": sibling},
            device_id_type=MESH,
        )

    def sum_copy(j, row, q):
        line = lax.div(j, 2)
        return pltpu.make_async_remote_copy(
            src_ref=part.at[j, row, piece(other * pieces + q), :],
            dst_ref=from_y.at[line, row, piece(q), :],
            send_sem=sum_send.at[line, row, q],
            recv_sem=sum_recv.at[line, row, q],
            device_id={"fs": beside},
            device_id_type=MESH,
        )

    def last_copy(j, row, q):
        return pltpu.make_async_remote_copy(
            src_ref=part.at[j, row, piece(why * pieces + q), :],
            dst_ref=from_x.at[row, piece(q), :],
            send_sem=last_send.at[row, q],
            recv_sem=last_recv.at[row, q],
            device_id={"tp": across},
            device_id_type=MESH,
        )

    def multiply(k, row, half):
        j = block_at(k)
        wide = h_back.shape[2]
        columns = pl.ds(pl.multiple_of((j * WIDTH + row) * wide, wide), wide)

        @pl.loop(0, pieces)
        def _(q):
            t = half * pieces + q
            term = jnp.dot(hidden[piece(t), :], back[:, columns], preferred_element_type=f32)
            part[j, row, piece(t), :] = (term * scales[8:9, columns]).astype(bf16)
            pl.when(core != lax.rem(j, 2))(lambda: core_copy(j, row, t).start())

    def added(j, row, t, extra):
        return part[j, row, piece(t), :].astype(f32) + extra.astype(f32)

    def reduce_core(k, row, half):
        j = block_at(k)

        @pl.when(core == lax.rem(j, 2))
        def _():
            line = lax.div(j, 2)
            for q in range(pieces):
                t = half * pieces + q
                core_copy(j, row, t).wait_recv()
                total = added(j, row, t, from_core[line, row, piece(t), :])
                part[j, row, piece(t), :] = total.astype(bf16)
                if half is other:
                    sum_copy(j, row, q).start()

    def reduce_y(k, row):
        j = block_at(k)

        @pl.when(core == lax.rem(j, 2))
        def _():
            line = lax.div(j, 2)
            for q in range(pieces):
                t = why * pieces + q
                sum_copy(j, row, q).wait_recv()
                total = added(j, row, t, from_y[line, row, piece(q), :])
                part[j, row, piece(t), :] = total.astype(bf16)
                pl.when(ex != line)(lambda: last_copy(j, row, q).start())

    def reduce_x(k, row):
        j = block_at(k)
        wide = h_back.shape[2]

        @pl.when(tp == j)
        def _():
            columns = pl.ds(row * wide, wide)
            for q in range(pieces):
                t = why * pieces + q
                last_copy(j, row, q).wait_recv()
                total = added(j, row, t, from_x[row, piece(q), :])
                kept = residual_own[piece(q), columns].astype(f32)
                out[piece(q), columns] = (kept + total).astype(bf16)

    for q in range(share):
        act_copy(other, 1 - core, q, 1).wait_recv()
    activate(other * count, tiles)
    for row in range(WIDTH):
        relay(BACK, 1, row)
    for row in range(WIDTH):
        multiply(0, row, other)
        reduce_core(0, row, other)
    activate(base, tiles)
    for row in range(WIDTH):
        relay(BACK, 2, row)
    for row in range(WIDTH):
        multiply(0, row, why)
        reduce_core(0, row, why)

    order = [(k, row) for k in range(DEPTH) for row in range(WIDTH)]
    for u, (k, row) in enumerate(order):
        if k:
            owner = block_at(k) * WIDTH + row
            pl.when(outer)(lambda: arrived(BACK, owner))
            for half in (other, why):
                multiply(k, row, half)
                reduce_core(k, row, half)
            if u == WIDTH:
                reduce_y(*order[0])
            reduce_y(*order[u - 1])
            reduce_x(*order[u - 2])
    reduce_y(*order[-1])
    reduce_x(*order[-2])
    reduce_x(*order[-1])

    def sent(p, row):
        owner = zed * WIDTH + row
        pl.when(can_up)(lambda: z_copy(p, owner, UP).wait_send())
        pl.when(can_down)(lambda: z_copy(p, owner, DOWN).wait_send())
        for s in (1, 2):
            low, high = (zed - s) * WIDTH + row, (zed + s) * WIDTH + row
            pl.when((zed >= s) & can_up)(lambda: z_copy(p, low, UP).wait_send())
            pl.when((zed + s <= last_z) & can_down)(lambda: z_copy(p, high, DOWN).wait_send())

    for p in range(5):
        sent(p, why)
        y_copy(p, me).wait_send()
        if p in (GATED, BACK):
            sent(p, other)
        else:
            for s in (1, 2, 3):
                low, high = (zed - s) * WIDTH + why, (zed + s) * WIDTH + why
                pl.when(zed >= s)(lambda: y_copy(p, low).wait_send())
                pl.when(zed + s <= last_z)(lambda: y_copy(p, high).wait_send())
    for owner in range(DEPTH * WIDTH):
        for k in range(3):
            mx_copy(owner, k).wait_send()
    for k in range(3):
        tp_copy(1, k).wait_send()
    for q in range(share):
        act_copy(why, core, q, 0).wait_send()
        act_copy(other, core, q, 1).wait_send()
    for j in range(DEPTH):
        for row in range(WIDTH):

            @pl.when(core != j % 2)
            def _():
                for t in range(WIDTH * pieces):
                    core_copy(j, row, t).wait_send()

            @pl.when(core == j % 2)
            def _():
                for q in range(pieces):
                    sum_copy(j, row, q).wait_send()
                    pl.when(ex != j // 2)(lambda: last_copy(j, row, q).wait_send())


def fused_device(
    tokens,
    mixer_gain,
    ffn_gain,
    w_outer,
    w_inner,
    w_value,
    scale_outer,
    scale_inner,
    scale_value,
    conv_taps,
    w_mixout,
    scale_mixout,
    w_gate,
    w_upward,
    scale_gate,
    scale_upward,
    w_down,
    scale_down,
):
    bf16 = jnp.bfloat16
    count, feat = tokens.shape
    model = mixer_gain.shape[0]
    chan = w_outer.shape[1]
    units = w_gate.shape[1]
    cols = w_down.shape[1]
    half = units // 2
    padded = half // 128 * 128 + 128
    vmem = pl.BlockSpec(memory_space=pltpu.VMEM)
    hbm = pl.BlockSpec(memory_space=pl.ANY)
    dma = pltpu.SemaphoreType.DMA
    owners = DEPTH * WIDTH
    return pl.pallas_call(
        block_kernel,
        out_shape=jax.ShapeDtypeStruct((count, feat), bf16),
        in_specs=[hbm if k in (12, 13, 16) else vmem for k in range(18)],
        out_specs=vmem,
        scratch_shapes=[
            pltpu.VMEM((16, cols), jnp.float32),
            pltpu.VMEM((w_outer.shape[0], 3 * chan), bf16),
            pltpu.VMEM(w_mixout.shape, bf16),
            pltpu.VMEM((2, w_gate.shape[0], units), bf16),
            pltpu.VMEM((2, half, cols), bf16),
            pltpu.VMEM((2, units), jnp.float32),
            pltpu.VMEM(w_gate.shape, jnp.float32),
            pltpu.VMEM(w_upward.shape, jnp.float32),
            pltpu.VMEM(w_down.shape, jnp.float32),
            pltpu.VMEM((WIDTH * count, model), bf16),
            pltpu.VMEM((model, 3 * chan), bf16),
            pltpu.VMEM((TP * chan, model), bf16),
            pltpu.VMEM((model, units), bf16),
            pltpu.VMEM((padded, model), bf16),
            pltpu.VMEM((16, model), jnp.float32),
            pltpu.VMEM((count, TP * chan), bf16),
            pltpu.VMEM((WIDTH * count, padded), bf16),
            pltpu.VMEM((count, feat), bf16),
            pltpu.VMEM((DEPTH, WIDTH, WIDTH * count, cols), bf16),
            pltpu.VMEM((2, WIDTH, WIDTH * count, cols), bf16),
            pltpu.VMEM((2, WIDTH, count, cols), bf16),
            pltpu.VMEM((WIDTH, count, cols), bf16),
            dma((5, owners, 2)),
            dma((5, owners)),
            dma((5, owners)),
            dma((2, 3)),
            dma((2, 3)),
            dma((owners, 3)),
            dma((owners, 3)),
            dma((2, 2)),
            dma((2, 2)),
            dma((2, WIDTH, 4)),
            dma((2, WIDTH, 4)),
            dma((2, WIDTH, 2)),
            dma((2, WIDTH, 2)),
            dma((WIDTH, 2)),
            dma((WIDTH, 2)),
            dma((9,)),
        ],
        compiler_params=pltpu.CompilerParams(
            collective_id=0, has_side_effects=True, vmem_limit_bytes=62 * 1024 * 1024
        ),
    )(
        tokens, mixer_gain[None], ffn_gain[None], w_outer, w_inner, w_value,
        scale_outer, scale_inner, scale_value, conv_taps, w_mixout, scale_mixout,
        w_gate, w_upward, scale_gate, scale_upward, w_down, scale_down,
    )


def plain_device(
    tokens,
    mixer_gain,
    ffn_gain,
    w_outer,
    w_inner,
    w_value,
    scale_outer,
    scale_inner,
    scale_value,
    conv_taps,
    w_mixout,
    scale_mixout,
    w_gate,
    w_upward,
    scale_gate,
    scale_upward,
    w_down,
    scale_down,
):
    full_rows = lax.all_gather(tokens, "tp", axis=1, tiled=True)
    normed = rms_scaled(full_rows, mixer_gain)
    tok_count = tokens.shape[0]
    local_channels = w_outer.shape[1]

    def add_one(w_piece):
        return add_rows(normed, w_piece)

    outer_bf = w_outer.astype(jnp.bfloat16)
    inner_bf = w_inner.astype(jnp.bfloat16)
    value_bf = w_value.astype(jnp.bfloat16)
    outer = add_one(lax.all_gather(outer_bf, "fs", axis=0, tiled=True))
    inner = add_one(lax.all_gather(inner_bf, "fs", axis=0, tiled=True))
    value = add_one(lax.all_gather(value_bf, "fs", axis=0, tiled=True))
    outer = outer * scale_outer
    product = inner * scale_inner * (value * scale_value)
    product = product.reshape(tok_count // SEQ_LEN, SEQ_LEN, local_channels)
    conv = causal_taps(product, conv_taps).reshape(tok_count, local_channels)
    mixed_out = (outer * conv).astype(jnp.bfloat16)
    mixout_scales, down_scales = (
        lax.all_gather(scale_mixout, "fs", axis=1, tiled=True),
        lax.all_gather(scale_down, "fs", axis=1, tiled=True),
    )
    mixout_bf = w_mixout.astype(jnp.bfloat16)
    mixed_all = lax.all_gather(mixed_out, "tp", axis=1, tiled=True)
    mixout_cols = lax.all_gather(mixout_bf, "fs", axis=1, tiled=True)
    mixout_all = lax.all_gather(mixout_cols, "tp", axis=0, tiled=True)
    mix_term = jnp.dot(mixed_all, mixout_all, preferred_element_type=jnp.float32) * mixout_scales
    residual_rows = (full_rows.astype(jnp.float32) + mix_term).astype(jnp.bfloat16)
    feature_count = tokens.shape[1]
    residual = lax.dynamic_slice_in_dim(
        residual_rows, lax.axis_index("tp") * feature_count, feature_count, 1
    )
    normed_ffn = rms_scaled(residual_rows, ffn_gain)
    gate_proj = add_rows(
        normed_ffn, lax.all_gather(w_gate.astype(jnp.bfloat16), "fs", axis=0, tiled=True)
    )
    up_proj = add_rows(
        normed_ffn, lax.all_gather(w_upward.astype(jnp.bfloat16), "fs", axis=0, tiled=True)
    )
    hidden = (jax.nn.silu(gate_proj * scale_gate) * (up_proj * scale_upward)).astype(jnp.bfloat16)
    down_terms = (
        jnp.dot(
            hidden,
            lax.all_gather(w_down.astype(jnp.bfloat16), "fs", axis=1, tiled=True),
            preferred_element_type=jnp.float32,
        )
        * down_scales
    )
    ffn_share = lax.psum_scatter(
        down_terms.astype(jnp.bfloat16), "tp", scatter_dimension=1, tiled=True
    ).astype(jnp.float32)
    return (residual.astype(jnp.float32) + ffn_share).astype(jnp.bfloat16)


def solution(mesh):
    in_specs = (
        P("fs", "tp"),
        P(),
        P(),
        P("fs", "tp"),
        P("fs", "tp"),
        P("fs", "tp"),
        P(None, "tp"),
        P(None, "tp"),
        P(None, "tp"),
        P(None, "tp"),
        P("tp", "fs"),
        P(None, "fs"),
        P("fs", "tp"),
        P("fs", "tp"),
        P(None, "tp"),
        P(None, "tp"),
        P("tp", "fs"),
        P(None, "fs"),
    )
    out_specs = P("fs", "tp")
    chosen = fused_device if (mesh.shape["fs"], mesh.shape["tp"]) == (8, 4) else plain_device
    return jax.shard_map(
        chosen, mesh=mesh, in_specs=in_specs, out_specs=out_specs, check_vma=False
    )
```

```python
import jax
import jax.numpy as jnp
from jax import lax
from jax.experimental import pallas as pl
from jax.experimental.pallas import tpu as pltpu
from jax.sharding import PartitionSpec as P

SEQ_LEN = 128


def rms_scaled(full_rows, gain_vec):
    values = full_rows.astype(jnp.float32)
    inverse = lax.rsqrt(jnp.mean(values * values, axis=-1, keepdims=True) + 1e-06)
    return (values * inverse * gain_vec).astype(jnp.bfloat16)


def add_rows(left, w_piece):
    return jnp.dot(left, w_piece, preferred_element_type=jnp.float32)


def causal_taps(product, conv_taps):
    padded = jnp.pad(product, ((0, 0), (conv_taps.shape[0] - 1, 0), (0, 0)))
    length = product.shape[1]
    summed = jnp.zeros(product.shape, jnp.float32)
    for tap_index in range(conv_taps.shape[0]):
        summed = summed + conv_taps[tap_index] * padded[:, tap_index : tap_index + length, :]
    return summed


DEPTH, WIDTH, TP = 4, 2, 4
ROWS = 256
PIECE = 512
UP, DOWN = 0, 1
SCALES, MIXER, MIXOUT, GATED, BACK = range(5)
MESH = pl.DeviceIdType.MESH


def block_kernel(
    tokens, mixer_gain, ffn_gain, w_outer, w_inner, w_value, s_outer, s_inner, s_value, taps,
    w_mixout, s_mixout, w_gate, w_upward, s_gate, s_upward, w_down, s_down,
    out,
    h_scales, h_mixer, h_mixout, h_gated, h_back, s_gated, raw_gate, raw_up, raw_down,
    act, mixer, mixout, gated, back, scales, mixed, hidden, residual_own,
    part, from_core, from_y, from_x,
    z_send, y_send, fs_recv, tp_send, tp_recv, mx_send, mx_recv,
    act_send, act_recv, core_send, core_recv, sum_send, sum_recv, last_send, last_recv,
    local_sem,
):
    f32, bf16 = jnp.float32, jnp.bfloat16
    me, tp = lax.axis_index("fs"), lax.axis_index("tp")
    zed, why = lax.div(me, WIDTH), lax.rem(me, WIDTH)
    ex, core = lax.div(tp, 2), lax.rem(tp, 2)
    other = 1 - why
    last_z = DEPTH - 1
    count = tokens.shape[0]
    tiles = count // ROWS

    beside = zed * WIDTH + other
    sibling = ex * 2 + (1 - core)
    across = (1 - ex) * 2 + core

    def fetch(k):
        source, target = ((w_gate, raw_gate), (w_upward, raw_up), (w_down, raw_down))[k]
        return pltpu.make_async_copy(source, target, local_sem.at[6 + k])

    for k in range(3):
        fetch(k).start()
    barrier = pltpu.get_barrier_semaphore()
    ring = [lax.rem(zed + step, DEPTH) * WIDTH + why for step in (1, DEPTH - 1)]
    for peer in (beside, *ring):
        pl.semaphore_signal(barrier, inc=1, device_id={"fs": peer}, device_id_type=MESH)
    for peer in (sibling, across):
        pl.semaphore_signal(barrier, inc=1, device_id={"tp": peer}, device_id_type=MESH)
    wide = w_outer.shape[1]
    for k, w in enumerate((w_outer, w_inner, w_value)):
        h_mixer[:, k * wide : (k + 1) * wide] = w[...].astype(bf16)
    h_mixout[...] = w_mixout[...].astype(bf16)
    for k, row in enumerate((s_mixout, s_down)):
        h_scales[k * 8 : (k + 1) * 8, :] = jnp.broadcast_to(row[...], (8, row.shape[1]))
    pl.semaphore_wait(barrier, 5)

    fulls = (scales, mixer, mixout, gated, back)
    own_src = (h_scales, h_mixer, h_mixout, h_gated.at[why], h_back.at[why])

    def place(p, owner):
        if p in (MIXER, GATED):
            height = own_src[p].shape[0]
            return fulls[p].at[pl.ds(pl.multiple_of(owner * height, height), height), :]
        height, wide = own_src[p].shape
        first = pl.multiple_of(tp * height, height) if p == MIXOUT else 0
        return fulls[p].at[pl.ds(first, height), pl.ds(pl.multiple_of(owner * wide, wide), wide)]

    def z_copy(p, owner, way, src=None):
        spot = place(p, owner)
        step = 1 if way == UP else -1
        return pltpu.make_async_remote_copy(
            src_ref=spot if src is None else src,
            dst_ref=spot,
            send_sem=z_send.at[p, owner, way],
            recv_sem=fs_recv.at[p, owner],
            device_id={"fs": (zed + step) * WIDTH + why},
            device_id_type=MESH,
        )

    def y_copy(p, owner, src=None):
        spot = place(p, owner)
        return pltpu.make_async_remote_copy(
            src_ref=spot if src is None else src,
            dst_ref=spot,
            send_sem=y_send.at[p, owner],
            recv_sem=fs_recv.at[p, owner],
            device_id={"fs": beside},
            device_id_type=MESH,
        )

    def arrived(p, owner):
        y_copy(p, owner).wait_recv()

    def own(p):
        return pltpu.make_async_copy(own_src[p], place(p, me), local_sem.at[p])

    can_up, can_down = zed < last_z, zed > 0
    outer = (zed == 0) | (zed == last_z)

    def z_own(p, row, src):
        owner = zed * WIDTH + row
        pl.when(can_up)(lambda: z_copy(p, owner, UP, src).start())
        pl.when(can_down)(lambda: z_copy(p, owner, DOWN, src).start())

    def relay(p, s, row):
        low, high = (zed - s) * WIDTH + row, (zed + s) * WIDTH + row

        @pl.when((zed >= s) & can_up)
        def _():
            arrived(p, low)
            z_copy(p, low, UP).start()

        @pl.when((zed + s <= last_z) & can_down)
        def _():
            arrived(p, high)
            z_copy(p, high, DOWN).start()

    def settle(p, s, row):
        low, high = (zed - s) * WIDTH + row, (zed + s) * WIDTH + row
        pl.when((zed >= s) & (zed == last_z))(lambda: arrived(p, low))
        pl.when((zed + s <= last_z) & (zed == 0))(lambda: arrived(p, high))

    def mx_copy(owner, k, src=None):
        line, target = ((tp, sibling), (tp, across), (across, sibling))[k]
        height, wide = h_mixout.shape
        spot = mixout.at[
            pl.ds(pl.multiple_of(line * height, height), height),
            pl.ds(pl.multiple_of(owner * wide, wide), wide),
        ]
        return pltpu.make_async_remote_copy(
            src_ref=spot if src is None else src,
            dst_ref=spot,
            send_sem=mx_send.at[owner, k],
            recv_sem=mx_recv.at[owner, k],
            device_id={"tp": target},
            device_id_type=MESH,
        )

    def mx_first(owner, src=None):
        mx_copy(owner, 1, src).start()
        mx_copy(owner, 0, src).start()

    firsts = (SCALES, MIXOUT, MIXER)

    def relay_first(s):
        low, high = (zed - s) * WIDTH + why, (zed + s) * WIDTH + why

        @pl.when(zed >= s)
        def _():
            for p in firsts:
                arrived(p, low)
                pl.when(can_up)(lambda: z_copy(p, low, UP).start())
                y_copy(p, low).start()
                if p == MIXOUT:
                    mx_first(low)

        @pl.when(zed + s <= last_z)
        def _():
            for p in firsts:
                arrived(p, high)
                pl.when(can_down)(lambda: z_copy(p, high, DOWN).start())
                y_copy(p, high).start()
                if p == MIXOUT:
                    mx_first(high)

    def from_beside(s):
        def take(owner):
            for p in firsts:
                arrived(p, owner)
                if p == MIXOUT:
                    mx_first(owner)

        if s == 0:
            take(beside)
            return
        low, high = (zed - s) * WIDTH + other, (zed + s) * WIDTH + other
        pl.when(zed >= s)(lambda: take(low))
        pl.when(zed + s <= last_z)(lambda: take(high))

    base = pl.multiple_of(why * count, count)

    def tp_slot(a, owner):
        if a == 0:
            wide = tokens.shape[1]
            return act.at[pl.ds(base, count), pl.ds(pl.multiple_of(owner * wide, wide), wide)]
        wide = mixed.shape[1] // TP
        return mixed.at[:, pl.ds(pl.multiple_of(owner * wide, wide), wide)]

    def tp_copy(a, k):
        owner, target = ((tp, sibling), (tp, across), (across, sibling))[k]
        spot = tp_slot(a, owner)
        return pltpu.make_async_remote_copy(
            src_ref=tokens if a == 0 and k < 2 else spot,
            dst_ref=spot,
            send_sem=tp_send.at[a, k],
            recv_sem=tp_recv.at[a, k],
            device_id={"tp": target},
            device_id_type=MESH,
        )

    def tp_first(a):
        tp_copy(a, 1).start()
        tp_copy(a, 0).start()

    def tp_second(a):
        tp_copy(a, 1).wait_recv()
        tp_copy(a, 2).start()

    def tp_finish(a):
        tp_copy(a, 0).wait_recv()
        tp_copy(a, 2).wait_recv()

    own_tokens = pltpu.make_async_copy(tokens, tp_slot(0, tp), local_sem.at[5])

    for p in firsts:
        y_copy(p, me, own_src[p]).start()
        z_own(p, why, own_src[p])
    tp_first(0)
    mx_first(me, h_mixout)
    own_tokens.start()
    for p in firsts:
        own(p).start()
    units = h_back.shape[1]
    main = units // 128 * 128
    middle, after = pl.ds(main, 128), main + 128

    def share_out(gate, up, write):
        write(0, pl.ds(0, main), gate[:, :main])
        write(0, pl.ds(after, main), up[:, :main])
        write(1, pl.ds(0, main), gate[:, after:])
        write(1, pl.ds(after, main), up[:, after:])
        gate, up = gate[:, middle], up[:, middle]
        low = lax.broadcasted_iota(jnp.int32, gate.shape, 1) < 64
        write(0, middle, jnp.where(low, gate, pltpu.roll(up, 64, 1)))
        write(1, middle, jnp.where(low, pltpu.roll(gate, 64, 1), up))

    def write_scale(half, lanes, values):
        s_gated[half : half + 1, lanes] = values

    def write_gated(half, lanes, values):
        h_gated[half, :, lanes] = values.astype(bf16)

    for k in range(3):
        fetch(k).wait()
    share_out(raw_gate, raw_up, write_gated)
    h_back[0] = raw_down[:units, :].astype(bf16)
    h_back[1, :main, :] = raw_down[after:, :].astype(bf16)
    h_back[1, main:, :] = raw_down[units:after, :].astype(bf16)
    spread = [jnp.broadcast_to(row[...], (8, row.shape[1])) for row in (s_gate, s_upward)]
    share_out(
        *spread, lambda half, lanes, values: write_scale(half, lanes, values[0:1])
    )
    for p in (GATED, BACK):
        own(p).start()
    back[units:, :] = jnp.zeros((back.shape[0] - units, back.shape[1]), bf16)

    relay_first(1)
    tp_second(0)
    relay_first(2)
    z_own(GATED, why, own_src[GATED])
    relay_first(3)
    y_copy(GATED, me, h_gated.at[other]).start()
    for s in range(DEPTH):
        from_beside(s)
    relay(GATED, 1, why)
    tp_finish(0)
    own_tokens.wait()
    for p in firsts:
        own(p).wait()

    chan = mixed.shape[1] // TP

    def tile(i):
        return pl.ds(pl.multiple_of(i * ROWS, ROWS), ROWS)

    def own_rows(i):
        return pl.ds(pl.multiple_of(base + i * ROWS, ROWS), ROWS)

    def normalised(values, gain):
        inverse = lax.rsqrt(jnp.mean(values * values, axis=-1, keepdims=True) + 1e-06)
        return (values * inverse * gain[...]).astype(bf16)

    @pl.loop(0, tiles)
    def _(i):
        normed = normalised(act[own_rows(i), :].astype(f32), mixer_gain)
        three = jnp.dot(normed, mixer[...], preferred_element_type=f32)
        product = (three[:, chan : 2 * chan] * s_inner[...]) * (three[:, 2 * chan :] * s_value[...])
        row = lax.rem(lax.broadcasted_iota(jnp.int32, product.shape, 0), SEQ_LEN)
        total = jnp.zeros_like(product)
        last = taps.shape[0] - 1
        for j in range(taps.shape[0]):
            gap = last - j
            moved = product
            if gap:
                moved = jnp.where(row >= gap, pltpu.roll(product, gap, 0), 0.0)
            total = total + taps[j : j + 1, :] * moved
        mixed[tile(i), pl.ds(pl.multiple_of(tp * chan, chan), chan)] = (
            three[:, :chan] * s_outer[...] * total
        ).astype(bf16)

    tp_first(1)
    relay(GATED, 2, why)
    arrived(GATED, beside)
    z_own(GATED, other, None)
    for owner in range(DEPTH * WIDTH):
        mx_copy(owner, 1).wait_recv()
        mx_copy(owner, 2).start()
    tp_second(1)
    relay(GATED, 1, other)
    for owner in range(DEPTH * WIDTH):
        mx_copy(owner, 0).wait_recv()
        mx_copy(owner, 2).wait_recv()
    tp_finish(1)
    for k in range(3):
        tp_copy(0, k).wait_send()

    feat = tokens.shape[1]
    quarter = count // TP
    strip = quarter // 2

    def act_copy(k, h):
        half, owner, target = (
            (why, tp, {"fs": beside}),
            (other, tp, {"tp": sibling}),
            (other, tp, {"tp": across}),
            (other, across, {"tp": sibling}),
        )[k]
        first = half * count + owner * quarter + h * strip
        spot = act.at[pl.ds(pl.multiple_of(first, strip), strip), :]
        return pltpu.make_async_remote_copy(
            src_ref=spot,
            dst_ref=spot,
            send_sem=act_send.at[k, h],
            recv_sem=act_recv.at[k, h],
            device_id=target,
            device_id_type=MESH,
        )

    @pl.loop(0, tiles)
    def _(step):
        i = lax.rem(step + tp, tiles)
        term = jnp.dot(mixed[tile(i), :], mixout[...], preferred_element_type=f32)
        term = term * scales[0:1, :]
        residual = (act[own_rows(i), :].astype(f32) + term).astype(bf16)
        act[own_rows(i), :] = residual
        residual_own[tile(i), :] = act[
            own_rows(i), pl.ds(pl.multiple_of(tp * feat, feat), feat)
        ]
        act[own_rows(i), :] = normalised(residual.astype(f32), ffn_gain)

        @pl.when(step == 0)
        def _():
            for h in range(2):
                act_copy(0, h).start()

    y_copy(BACK, me, h_back.at[other]).start()

    def spread_act(h):
        act_copy(0, h).wait_recv()
        act_copy(2, h).start()
        act_copy(1, h).start()

    spread_act(0)
    relay(GATED, 2, other)
    spread_act(1)
    arrived(BACK, beside)
    own(BACK).wait()
    for row in range(WIDTH):
        z_own(BACK, row, None)
    for h in range(2):
        act_copy(2, h).wait_recv()
        act_copy(3, h).start()
    own(GATED).wait()
    for row in (why, other):
        for s in (1, 2, 3):
            settle(GATED, s, row)

    def activate(first, steps):
        @pl.loop(0, steps)
        def _(i):
            rows = pl.ds(pl.multiple_of(first + i * ROWS, ROWS), ROWS)
            both = jnp.dot(act[rows, :], gated[...], preferred_element_type=f32)
            both = both * s_gated[pl.ds(why, 1), :]
            gate, up = both[:, :main], both[:, main + 128 :]
            hidden[rows, :main] = (gate / (1.0 + jnp.exp(-gate)) * up).astype(bf16)
            gate = both[:, main : main + 128]
            up = pltpu.roll(gate, 64, 1)
            rest = gate / (1.0 + jnp.exp(-gate)) * up
            lane = lax.broadcasted_iota(jnp.int32, rest.shape, 1)
            hidden[rows, main:] = jnp.where(lane < 64, rest, 0.0).astype(bf16)

    pieces = count // PIECE

    def piece(t):
        return pl.ds(pl.multiple_of(t * PIECE, PIECE), PIECE)

    def block_at(k):
        return lax.rem(zed + k * (1 - 2 * lax.div(zed, last_z)) + DEPTH, DEPTH)

    def core_copy(j, row, t):
        line = lax.div(j, 2)
        return pltpu.make_async_remote_copy(
            src_ref=part.at[j, row, piece(t), :],
            dst_ref=from_core.at[line, row, piece(t), :],
            send_sem=core_send.at[line, row, t],
            recv_sem=core_recv.at[line, row, t],
            device_id={"tp": sibling},
            device_id_type=MESH,
        )

    def sum_copy(j, row, q):
        line = lax.div(j, 2)
        return pltpu.make_async_remote_copy(
            src_ref=part.at[j, row, piece(other * pieces + q), :],
            dst_ref=from_y.at[line, row, piece(q), :],
            send_sem=sum_send.at[line, row, q],
            recv_sem=sum_recv.at[line, row, q],
            device_id={"fs": beside},
            device_id_type=MESH,
        )

    def last_copy(j, row, t):
        return pltpu.make_async_remote_copy(
            src_ref=part.at[j, row, piece(t), :],
            dst_ref=from_x.at[row, piece(t), :],
            send_sem=last_send.at[row, t],
            recv_sem=last_recv.at[row, t],
            device_id={"tp": across},
            device_id_type=MESH,
        )

    def x_first(k, row):
        return row == 0 and k < last_z

    def multiply(k, row, half):
        j = block_at(k)
        wide = h_back.shape[2]
        columns = pl.ds(pl.multiple_of((j * WIDTH + row) * wide, wide), wide)

        @pl.loop(0, pieces)
        def _(q):
            t = half * pieces + q
            term = jnp.dot(hidden[piece(t), :], back[:, columns], preferred_element_type=f32)
            part[j, row, piece(t), :] = (term * scales[8:9, columns]).astype(bf16)
            pl.when(core != lax.rem(j, 2))(lambda: core_copy(j, row, t).start())

    def added(j, row, t, extra):
        return part[j, row, piece(t), :].astype(f32) + extra.astype(f32)

    def stage_1(k, row, half):
        j = block_at(k)

        @pl.when(core == lax.rem(j, 2))
        def _():
            line = lax.div(j, 2)
            for q in range(pieces):
                t = half * pieces + q
                core_copy(j, row, t).wait_recv()
                total = added(j, row, t, from_core[line, row, piece(t), :])
                part[j, row, piece(t), :] = total.astype(bf16)
                if x_first(k, row):
                    pl.when(ex != line)(lambda: last_copy(j, row, t).start())
                elif half is other:
                    sum_copy(j, row, q).start()

    def stage_2(k, row):
        j = block_at(k)
        line = lax.div(j, 2)
        mine = core == lax.rem(j, 2)

        def x_sums():
            for half in (other, why):
                for q in range(pieces):
                    t = half * pieces + q
                    last_copy(j, row, t).wait_recv()
                    total = added(j, row, t, from_x[row, piece(t), :])
                    part[j, row, piece(t), :] = total.astype(bf16)
                    if half is other:
                        sum_copy(j, row, q).start()

        def y_sums():
            for q in range(pieces):
                t = why * pieces + q
                sum_copy(j, row, q).wait_recv()
                total = added(j, row, t, from_y[line, row, piece(q), :])
                part[j, row, piece(t), :] = total.astype(bf16)
                pl.when(ex != line)(lambda: last_copy(j, row, t).start())

        if x_first(k, row):
            pl.when(mine & (ex == line))(x_sums)
        else:
            pl.when(mine)(y_sums)

    def stage_3(k, row):
        j = block_at(k)
        wide = h_back.shape[2]

        @pl.when(tp == j)
        def _():
            columns = pl.ds(row * wide, wide)
            for q in range(pieces):
                t = why * pieces + q
                if x_first(k, row):
                    sum_copy(j, row, q).wait_recv()
                    extra = from_y[lax.div(j, 2), row, piece(q), :]
                else:
                    last_copy(j, row, t).wait_recv()
                    extra = from_x[row, piece(t), :]
                kept = residual_own[piece(q), columns].astype(f32)
                out[piece(q), columns] = (kept + added(j, row, t, extra)).astype(bf16)

    for h in range(2):
        act_copy(1, h).wait_recv()
        act_copy(3, h).wait_recv()
    activate(other * count, tiles)
    for row in range(WIDTH):
        relay(BACK, 1, row)
    for row in range(WIDTH):
        multiply(0, row, other)
        stage_1(0, row, other)
    activate(base, tiles)
    for row in range(WIDTH):
        relay(BACK, 2, row)
    for row in range(WIDTH):
        multiply(0, row, why)
        stage_1(0, row, why)

    order = [(k, row) for k in range(DEPTH) for row in range(WIDTH)]
    after_unit = {
        3: ((stage_2, 1), (stage_2, 0)),
        4: ((stage_2, 3),),
        5: ((stage_2, 2), (stage_3, 1), (stage_3, 0)),
        6: ((stage_2, 5), (stage_2, 4), (stage_3, 3)),
        7: (
            (stage_2, 6), (stage_3, 2), (stage_2, 7), (stage_3, 5), (stage_3, 4), (stage_3, 6),
            (stage_3, 7),
        ),
    }
    for u, (k, row) in enumerate(order):
        if k:
            owner = block_at(k) * WIDTH + row
            pl.when(outer)(lambda: arrived(BACK, owner))
            for half in (other, why):
                multiply(k, row, half)
                stage_1(k, row, half)
        for stage, unit in after_unit.get(u, ()):
            stage(*order[unit])

    def sent(p, row):
        owner = zed * WIDTH + row
        pl.when(can_up)(lambda: z_copy(p, owner, UP).wait_send())
        pl.when(can_down)(lambda: z_copy(p, owner, DOWN).wait_send())
        for s in (1, 2):
            low, high = (zed - s) * WIDTH + row, (zed + s) * WIDTH + row
            pl.when((zed >= s) & can_up)(lambda: z_copy(p, low, UP).wait_send())
            pl.when((zed + s <= last_z) & can_down)(lambda: z_copy(p, high, DOWN).wait_send())

    for p in range(5):
        sent(p, why)
        y_copy(p, me).wait_send()
        if p in (GATED, BACK):
            sent(p, other)
        else:
            for s in (1, 2, 3):
                low, high = (zed - s) * WIDTH + why, (zed + s) * WIDTH + why
                pl.when(zed >= s)(lambda: y_copy(p, low).wait_send())
                pl.when(zed + s <= last_z)(lambda: y_copy(p, high).wait_send())
    for owner in range(DEPTH * WIDTH):
        for k in range(3):
            mx_copy(owner, k).wait_send()
    for k in range(3):
        tp_copy(1, k).wait_send()
    for k in range(4):
        for h in range(2):
            act_copy(k, h).wait_send()
    for k, row in order:
        j = block_at(k)
        line = lax.div(j, 2)
        mine = core == lax.rem(j, 2)

        @pl.when(core != lax.rem(j, 2))
        def _():
            for t in range(WIDTH * pieces):
                core_copy(j, row, t).wait_send()

        def sums_sent():
            for q in range(pieces):
                sum_copy(j, row, q).wait_send()

        def lasts_sent(halves):
            for half in halves:
                for q in range(pieces):
                    last_copy(j, row, half * pieces + q).wait_send()

        first = x_first(k, row)
        pl.when(mine & (ex == line) if first else mine)(sums_sent)
        pl.when(mine & (ex != line))(lambda: lasts_sent((other, why) if first else (why,)))


def fused_device(
    tokens,
    mixer_gain,
    ffn_gain,
    w_outer,
    w_inner,
    w_value,
    scale_outer,
    scale_inner,
    scale_value,
    conv_taps,
    w_mixout,
    scale_mixout,
    w_gate,
    w_upward,
    scale_gate,
    scale_upward,
    w_down,
    scale_down,
):
    bf16 = jnp.bfloat16
    count, feat = tokens.shape
    model = mixer_gain.shape[0]
    chan = w_outer.shape[1]
    units = w_gate.shape[1]
    cols = w_down.shape[1]
    half = units // 2
    padded = half // 128 * 128 + 128
    vmem = pl.BlockSpec(memory_space=pltpu.VMEM)
    hbm = pl.BlockSpec(memory_space=pl.ANY)
    dma = pltpu.SemaphoreType.DMA
    owners = DEPTH * WIDTH
    return pl.pallas_call(
        block_kernel,
        out_shape=jax.ShapeDtypeStruct((count, feat), bf16),
        in_specs=[hbm if k in (12, 13, 16) else vmem for k in range(18)],
        out_specs=vmem,
        scratch_shapes=[
            pltpu.VMEM((16, cols), jnp.float32),
            pltpu.VMEM((w_outer.shape[0], 3 * chan), bf16),
            pltpu.VMEM(w_mixout.shape, bf16),
            pltpu.VMEM((2, w_gate.shape[0], units), bf16),
            pltpu.VMEM((2, half, cols), bf16),
            pltpu.VMEM((2, units), jnp.float32),
            pltpu.VMEM(w_gate.shape, jnp.float32),
            pltpu.VMEM(w_upward.shape, jnp.float32),
            pltpu.VMEM(w_down.shape, jnp.float32),
            pltpu.VMEM((WIDTH * count, model), bf16),
            pltpu.VMEM((model, 3 * chan), bf16),
            pltpu.VMEM((TP * chan, model), bf16),
            pltpu.VMEM((model, units), bf16),
            pltpu.VMEM((padded, model), bf16),
            pltpu.VMEM((16, model), jnp.float32),
            pltpu.VMEM((count, TP * chan), bf16),
            pltpu.VMEM((WIDTH * count, padded), bf16),
            pltpu.VMEM((count, feat), bf16),
            pltpu.VMEM((DEPTH, WIDTH, WIDTH * count, cols), bf16),
            pltpu.VMEM((2, WIDTH, WIDTH * count, cols), bf16),
            pltpu.VMEM((2, WIDTH, count, cols), bf16),
            pltpu.VMEM((WIDTH, WIDTH * count, cols), bf16),
            dma((5, owners, 2)),
            dma((5, owners)),
            dma((5, owners)),
            dma((2, 3)),
            dma((2, 3)),
            dma((owners, 3)),
            dma((owners, 3)),
            dma((4, 2)),
            dma((4, 2)),
            dma((2, WIDTH, 4)),
            dma((2, WIDTH, 4)),
            dma((2, WIDTH, 2)),
            dma((2, WIDTH, 2)),
            dma((WIDTH, 4)),
            dma((WIDTH, 4)),
            dma((9,)),
        ],
        compiler_params=pltpu.CompilerParams(
            collective_id=0, has_side_effects=True, vmem_limit_bytes=62 * 1024 * 1024
        ),
    )(
        tokens, mixer_gain[None], ffn_gain[None], w_outer, w_inner, w_value,
        scale_outer, scale_inner, scale_value, conv_taps, w_mixout, scale_mixout,
        w_gate, w_upward, scale_gate, scale_upward, w_down, scale_down,
    )


def plain_device(
    tokens,
    mixer_gain,
    ffn_gain,
    w_outer,
    w_inner,
    w_value,
    scale_outer,
    scale_inner,
    scale_value,
    conv_taps,
    w_mixout,
    scale_mixout,
    w_gate,
    w_upward,
    scale_gate,
    scale_upward,
    w_down,
    scale_down,
):
    full_rows = lax.all_gather(tokens, "tp", axis=1, tiled=True)
    normed = rms_scaled(full_rows, mixer_gain)
    tok_count = tokens.shape[0]
    local_channels = w_outer.shape[1]

    def add_one(w_piece):
        return add_rows(normed, w_piece)

    outer_bf = w_outer.astype(jnp.bfloat16)
    inner_bf = w_inner.astype(jnp.bfloat16)
    value_bf = w_value.astype(jnp.bfloat16)
    outer = add_one(lax.all_gather(outer_bf, "fs", axis=0, tiled=True))
    inner = add_one(lax.all_gather(inner_bf, "fs", axis=0, tiled=True))
    value = add_one(lax.all_gather(value_bf, "fs", axis=0, tiled=True))
    outer = outer * scale_outer
    product = inner * scale_inner * (value * scale_value)
    product = product.reshape(tok_count // SEQ_LEN, SEQ_LEN, local_channels)
    conv = causal_taps(product, conv_taps).reshape(tok_count, local_channels)
    mixed_out = (outer * conv).astype(jnp.bfloat16)
    mixout_scales, down_scales = (
        lax.all_gather(scale_mixout, "fs", axis=1, tiled=True),
        lax.all_gather(scale_down, "fs", axis=1, tiled=True),
    )
    mixout_bf = w_mixout.astype(jnp.bfloat16)
    mixed_all = lax.all_gather(mixed_out, "tp", axis=1, tiled=True)
    mixout_cols = lax.all_gather(mixout_bf, "fs", axis=1, tiled=True)
    mixout_all = lax.all_gather(mixout_cols, "tp", axis=0, tiled=True)
    mix_term = jnp.dot(mixed_all, mixout_all, preferred_element_type=jnp.float32) * mixout_scales
    residual_rows = (full_rows.astype(jnp.float32) + mix_term).astype(jnp.bfloat16)
    feature_count = tokens.shape[1]
    residual = lax.dynamic_slice_in_dim(
        residual_rows, lax.axis_index("tp") * feature_count, feature_count, 1
    )
    normed_ffn = rms_scaled(residual_rows, ffn_gain)
    gate_proj = add_rows(
        normed_ffn, lax.all_gather(w_gate.astype(jnp.bfloat16), "fs", axis=0, tiled=True)
    )
    up_proj = add_rows(
        normed_ffn, lax.all_gather(w_upward.astype(jnp.bfloat16), "fs", axis=0, tiled=True)
    )
    hidden = (jax.nn.silu(gate_proj * scale_gate) * (up_proj * scale_upward)).astype(jnp.bfloat16)
    down_terms = (
        jnp.dot(
            hidden,
            lax.all_gather(w_down.astype(jnp.bfloat16), "fs", axis=1, tiled=True),
            preferred_element_type=jnp.float32,
        )
        * down_scales
    )
    ffn_share = lax.psum_scatter(
        down_terms.astype(jnp.bfloat16), "tp", scatter_dimension=1, tiled=True
    ).astype(jnp.float32)
    return (residual.astype(jnp.float32) + ffn_share).astype(jnp.bfloat16)


def solution(mesh):
    in_specs = (
        P("fs", "tp"),
        P(),
        P(),
        P("fs", "tp"),
        P("fs", "tp"),
        P("fs", "tp"),
        P(None, "tp"),
        P(None, "tp"),
        P(None, "tp"),
        P(None, "tp"),
        P("tp", "fs"),
        P(None, "fs"),
        P("fs", "tp"),
        P("fs", "tp"),
        P(None, "tp"),
        P(None, "tp"),
        P("tp", "fs"),
        P(None, "fs"),
    )
    out_specs = P("fs", "tp")
    chosen = fused_device if (mesh.shape["fs"], mesh.shape["tp"]) == (8, 4) else plain_device
    return jax.shard_map(
        chosen, mesh=mesh, in_specs=in_specs, out_specs=out_specs, check_vma=False
    )
```

```python
import jax
import jax.numpy as jnp
from jax import lax
from jax.experimental import pallas as pl
from jax.experimental.pallas import tpu as pltpu
from jax.sharding import PartitionSpec as P

SEQ_LEN = 128


def rms_scaled(full_rows, gain_vec):
    values = full_rows.astype(jnp.float32)
    inverse = lax.rsqrt(jnp.mean(values * values, axis=-1, keepdims=True) + 1e-06)
    return (values * inverse * gain_vec).astype(jnp.bfloat16)


def add_rows(left, w_piece):
    return jnp.dot(left, w_piece, preferred_element_type=jnp.float32)


def causal_taps(product, conv_taps):
    padded = jnp.pad(product, ((0, 0), (conv_taps.shape[0] - 1, 0), (0, 0)))
    length = product.shape[1]
    summed = jnp.zeros(product.shape, jnp.float32)
    for tap_index in range(conv_taps.shape[0]):
        summed = summed + conv_taps[tap_index] * padded[:, tap_index : tap_index + length, :]
    return summed


DEPTH, WIDTH, TP = 4, 2, 4
ROWS = 256
PIECE = 512
UP, DOWN = 0, 1
SCALES, MIXER, MIXOUT, LEAD, REST, BACK = range(6)
MESH = pl.DeviceIdType.MESH


def block_kernel(
    tokens, mixer_gain, ffn_gain, w_outer, w_inner, w_value, s_outer, s_inner, s_value, taps,
    w_mixout, s_mixout, w_gate, w_upward, s_gate, s_upward, w_down, s_down,
    out,
    h_scales, h_mixer, h_mixout, h_lead, h_rest, h_back, s_lead, s_rest, raw_gate, raw_up, raw_down,
    raw_mixer, raw_mixout, raw_scale,
    act, mixer, mixout, lead, rest, back, scales, mixed, hidden, residual_own,
    part, from_core, from_y, from_x,
    z_send, y_send, fs_recv, tp_send, tp_recv, mx_send, mx_recv, mx_whole,
    act_send, act_recv, core_send, core_recv, sum_send, sum_recv, last_send, last_recv,
    local_sem,
):
    f32, bf16 = jnp.float32, jnp.bfloat16
    me, tp = lax.axis_index("fs"), lax.axis_index("tp")
    zed, why = lax.div(me, WIDTH), lax.rem(me, WIDTH)
    ex, core = lax.div(tp, 2), lax.rem(tp, 2)
    other = 1 - why
    last_z = DEPTH - 1
    count = tokens.shape[0]
    tiles = count // ROWS

    beside = zed * WIDTH + other
    sibling = ex * 2 + (1 - core)
    across = (1 - ex) * 2 + core

    wide = w_outer.shape[1]
    fetched = (
        (w_outer, raw_mixer.at[0]), (w_inner, raw_mixer.at[1]), (w_value, raw_mixer.at[2]),
        (w_mixout, raw_mixout), (w_gate, raw_gate), (w_upward, raw_up), (w_down, raw_down),
    )

    def fetch(k):
        return pltpu.make_async_copy(*fetched[k], local_sem.at[7 + k])

    for k in range(len(fetched)):
        fetch(k).start()
    barrier = pltpu.get_barrier_semaphore()
    ring = [lax.rem(zed + step, DEPTH) * WIDTH + why for step in (1, DEPTH - 1)]
    for peer in (beside, *ring):
        pl.semaphore_signal(barrier, inc=1, device_id={"fs": peer}, device_id_type=MESH)
    for peer in (sibling, across):
        pl.semaphore_signal(barrier, inc=1, device_id={"tp": peer}, device_id_type=MESH)
    for k in range(4):
        fetch(k).wait()
    for k in range(3):
        h_mixer[:, k * wide : (k + 1) * wide] = raw_mixer[k].astype(bf16)
    h_mixout[...] = raw_mixout[...].astype(bf16)
    for k, row in enumerate((s_mixout, s_down)):
        h_scales[k * 8 : (k + 1) * 8, :] = jnp.broadcast_to(row[...], (8, row.shape[1]))
    pl.semaphore_wait(barrier, 5)

    fulls = (scales, mixer, mixout, lead, rest, back)
    split = (h_lead, h_rest, h_back)
    own_src = (h_scales, h_mixer, h_mixout, *[h.at[why] for h in split])

    def place(p, owner):
        if p in (MIXER, LEAD, REST):
            height = own_src[p].shape[0]
            return fulls[p].at[pl.ds(pl.multiple_of(owner * height, height), height), :]
        height, wide = own_src[p].shape
        first = pl.multiple_of(tp * height, height) if p == MIXOUT else 0
        return fulls[p].at[pl.ds(first, height), pl.ds(pl.multiple_of(owner * wide, wide), wide)]

    first_own = LEAD * DEPTH - LEAD

    def kind(p, owner):
        return p if p < LEAD else LEAD + (p - LEAD) * WIDTH + lax.rem(owner, WIDTH)

    def line_of(owner, way):
        z = lax.div(owner, WIDTH)
        return z if way == UP else lax.select(z == zed, DEPTH, z)

    def z_copy(p, owner, way, src=None):
        spot = place(p, owner)
        step = 1 if way == UP else -1
        return pltpu.make_async_remote_copy(
            src_ref=spot if src is None else src,
            dst_ref=spot,
            send_sem=z_send.at[kind(p, owner), line_of(owner, way)],
            recv_sem=fs_recv.at[p, owner],
            device_id={"fs": (zed + step) * WIDTH + why},
            device_id_type=MESH,
        )

    def y_copy(p, owner, src=None):
        spot = place(p, owner)
        return pltpu.make_async_remote_copy(
            src_ref=spot if src is None else src,
            dst_ref=spot,
            send_sem=y_send.at[p * DEPTH + lax.div(owner, WIDTH) if p < LEAD else first_own + p],
            recv_sem=fs_recv.at[p, owner],
            device_id={"fs": beside},
            device_id_type=MESH,
        )

    def arrived(p, owner):
        y_copy(p, owner).wait_recv()

    def own(p):
        return pltpu.make_async_copy(own_src[p], place(p, me), local_sem.at[p])

    can_up, can_down = zed < last_z, zed > 0
    outer = (zed == 0) | (zed == last_z)

    def z_own(p, row, src):
        owner = zed * WIDTH + row
        pl.when(can_up)(lambda: z_copy(p, owner, UP, src).start())
        pl.when(can_down)(lambda: z_copy(p, owner, DOWN, src).start())

    def relay(p, s, row):
        low, high = (zed - s) * WIDTH + row, (zed + s) * WIDTH + row

        @pl.when((zed >= s) & can_up)
        def _():
            arrived(p, low)
            z_copy(p, low, UP).start()

        @pl.when((zed + s <= last_z) & can_down)
        def _():
            arrived(p, high)
            z_copy(p, high, DOWN).start()

    def settle(p, s, row):
        low, high = (zed - s) * WIDTH + row, (zed + s) * WIDTH + row
        pl.when((zed >= s) & (zed == last_z))(lambda: arrived(p, low))
        pl.when((zed + s <= last_z) & (zed == 0))(lambda: arrived(p, high))

    def mx_copy(owner, k, src=None):
        line, target = ((tp, sibling), (tp, across), (across, sibling))[k]
        height, wide = h_mixout.shape
        columns = slice(None)
        if owner is not None:
            columns = pl.ds(pl.multiple_of(owner * wide, wide), wide)
        spot = mixout.at[pl.ds(pl.multiple_of(line * height, height), height), columns]
        return pltpu.make_async_remote_copy(
            src_ref=spot if src is None else src,
            dst_ref=spot,
            send_sem=mx_send.at[k],
            recv_sem=mx_recv.at[0 if owner is None else owner] if k == 1 else mx_whole.at[k // 2],
            device_id={"tp": target},
            device_id_type=MESH,
        )

    def mx_first(owner, src=None):
        mx_copy(owner, 1, src).start()
        mx_copy(owner, 0, src).start()

    firsts = (SCALES, MIXOUT, MIXER)

    def relay_first(s):
        low, high = (zed - s) * WIDTH + why, (zed + s) * WIDTH + why

        @pl.when(zed >= s)
        def _():
            for p in firsts:
                arrived(p, low)
                pl.when(can_up)(lambda: z_copy(p, low, UP).start())
                y_copy(p, low).start()
                if p == MIXOUT:
                    mx_first(low)

        @pl.when(zed + s <= last_z)
        def _():
            for p in firsts:
                arrived(p, high)
                pl.when(can_down)(lambda: z_copy(p, high, DOWN).start())
                y_copy(p, high).start()
                if p == MIXOUT:
                    mx_first(high)

    def from_beside(s):
        def take(owner):
            for p in firsts:
                arrived(p, owner)
                if p == MIXOUT:
                    mx_first(owner)

        if s == 0:
            take(beside)
            return
        low, high = (zed - s) * WIDTH + other, (zed + s) * WIDTH + other
        pl.when(zed >= s)(lambda: take(low))
        pl.when(zed + s <= last_z)(lambda: take(high))

    base = pl.multiple_of(why * count, count)

    def tp_slot(a, owner):
        if a == 0:
            wide = tokens.shape[1]
            return act.at[pl.ds(base, count), pl.ds(pl.multiple_of(owner * wide, wide), wide)]
        wide = mixed.shape[1] // TP
        return mixed.at[:, pl.ds(pl.multiple_of(owner * wide, wide), wide)]

    def tp_copy(a, k):
        owner, target = ((tp, sibling), (tp, across), (across, sibling))[k]
        spot = tp_slot(a, owner)
        return pltpu.make_async_remote_copy(
            src_ref=tokens if a == 0 and k < 2 else spot,
            dst_ref=spot,
            send_sem=tp_send.at[a, k],
            recv_sem=tp_recv.at[a, k],
            device_id={"tp": target},
            device_id_type=MESH,
        )

    def tp_first(a):
        tp_copy(a, 1).start()
        tp_copy(a, 0).start()

    def tp_second(a):
        tp_copy(a, 1).wait_recv()
        tp_copy(a, 2).start()

    def tp_finish(a):
        tp_copy(a, 0).wait_recv()
        tp_copy(a, 2).wait_recv()

    own_tokens = pltpu.make_async_copy(tokens, tp_slot(0, tp), local_sem.at[6])

    for p in firsts:
        y_copy(p, me, own_src[p]).start()
        z_own(p, why, own_src[p])
    tp_first(0)
    mx_first(me, h_mixout)
    own_tokens.start()
    for p in firsts:
        own(p).start()
    units = h_back.shape[1]
    main = units // 128 * 128
    middle, after = pl.ds(main, 128), main + 128

    cut = h_lead.shape[2] // 2

    def share_out(gate, up, write):
        tail = main - cut
        for half, first in enumerate((0, after)):
            for k, source in enumerate((gate, up)):
                write(0, half, pl.ds(k * cut, cut), source[:, pl.ds(first, cut)])
                at = pl.ds(k * (tail + 128), tail)
                write(1, half, at, source[:, pl.ds(first + cut, tail)])
        gate, up = gate[:, middle], up[:, middle]
        low = lax.broadcasted_iota(jnp.int32, gate.shape, 1) < 64
        write(1, 0, pl.ds(tail, 128), jnp.where(low, gate, pltpu.roll(up, 64, 1)))
        write(1, 1, pl.ds(tail, 128), jnp.where(low, pltpu.roll(gate, 64, 1), up))

    def write_scale(target, half, lanes, values):
        (s_lead, s_rest)[target][half : half + 1, lanes] = values[0:1]

    def write_gated(target, half, lanes, values):
        split[target][half, :, lanes] = values.astype(bf16)

    for k in range(4, len(fetched)):
        fetch(k).wait()
    share_out(raw_gate, raw_up, write_gated)
    h_back[0] = raw_down[:units, :].astype(bf16)
    h_back[1, :main, :] = raw_down[after:, :].astype(bf16)
    h_back[1, main:, :] = raw_down[units:after, :].astype(bf16)
    for k, row in enumerate((s_gate, s_upward)):
        raw_scale[k] = jnp.broadcast_to(row[...], raw_scale.shape[1:])
    share_out(raw_scale.at[0], raw_scale.at[1], write_scale)
    for p in (LEAD, REST, BACK):
        own(p).start()
    back[units:, :] = jnp.zeros((back.shape[0] - units, back.shape[1]), bf16)

    @pl.when(outer)
    def _():
        for p in (LEAD, REST):
            z_own(p, why, own_src[p])

    relay_first(1)
    tp_second(0)
    relay_first(2)
    pl.when(jnp.logical_not(outer))(lambda: z_own(LEAD, why, own_src[LEAD]))
    relay_first(3)
    y_copy(LEAD, me, h_lead.at[other]).start()
    y_copy(REST, me, h_rest.at[other]).start()
    relay(LEAD, 1, why)
    for s in range(DEPTH):
        from_beside(s)
    relay(LEAD, 2, why)
    tp_finish(0)
    own_tokens.wait()
    for p in firsts:
        own(p).wait()

    chan = mixed.shape[1] // TP

    def tile(i):
        return pl.ds(pl.multiple_of(i * ROWS, ROWS), ROWS)

    def own_rows(i):
        return pl.ds(pl.multiple_of(base + i * ROWS, ROWS), ROWS)

    def normalised(values, gain):
        inverse = lax.rsqrt(jnp.mean(values * values, axis=-1, keepdims=True) + 1e-06)
        return (values * inverse * gain[...]).astype(bf16)

    @pl.loop(0, tiles)
    def _(i):
        normed = normalised(act[own_rows(i), :].astype(f32), mixer_gain)
        three = jnp.dot(normed, mixer[...], preferred_element_type=f32)
        product = (three[:, chan : 2 * chan] * s_inner[...]) * (three[:, 2 * chan :] * s_value[...])
        row = lax.rem(lax.broadcasted_iota(jnp.int32, product.shape, 0), SEQ_LEN)
        total = jnp.zeros_like(product)
        last = taps.shape[0] - 1
        for j in range(taps.shape[0]):
            gap = last - j
            moved = product
            if gap:
                moved = jnp.where(row >= gap, pltpu.roll(product, gap, 0), 0.0)
            total = total + taps[j : j + 1, :] * moved
        mixed[tile(i), pl.ds(pl.multiple_of(tp * chan, chan), chan)] = (
            three[:, :chan] * s_outer[...] * total
        ).astype(bf16)

    tp_first(1)
    arrived(LEAD, beside)
    z_own(LEAD, other, None)
    pl.when(jnp.logical_not(outer))(lambda: z_own(REST, why, own_src[REST]))
    for owner in range(DEPTH * WIDTH):
        mx_copy(owner, 1).wait_recv()
        mx_copy(owner, 2).start()
    tp_second(1)
    relay(LEAD, 1, other)
    mx_copy(None, 0).wait_recv()
    mx_copy(None, 2).wait_recv()
    tp_finish(1)
    for k in range(3):
        tp_copy(0, k).wait_send()

    arrived(REST, beside)
    z_own(REST, other, None)

    feat = tokens.shape[1]
    quarter = count // TP
    strip = quarter // 2

    def act_copy(k, h):
        half, owner, target = (
            (why, tp, {"fs": beside}),
            (other, tp, {"tp": sibling}),
            (other, tp, {"tp": across}),
            (other, across, {"tp": sibling}),
        )[k]
        first = half * count + owner * quarter + h * strip
        spot = act.at[pl.ds(pl.multiple_of(first, strip), strip), :]
        return pltpu.make_async_remote_copy(
            src_ref=spot,
            dst_ref=spot,
            send_sem=act_send.at[k, h],
            recv_sem=act_recv.at[k, h],
            device_id=target,
            device_id_type=MESH,
        )

    @pl.loop(0, tiles)
    def _(step):
        i = lax.rem(step + tp, tiles)
        term = jnp.dot(mixed[tile(i), :], mixout[...], preferred_element_type=f32)
        term = term * scales[0:1, :]
        residual = (act[own_rows(i), :].astype(f32) + term).astype(bf16)
        act[own_rows(i), :] = residual
        residual_own[tile(i), :] = act[
            own_rows(i), pl.ds(pl.multiple_of(tp * feat, feat), feat)
        ]
        act[own_rows(i), :] = normalised(residual.astype(f32), ffn_gain)

        @pl.when(step == 0)
        def _():
            for h in range(2):
                act_copy(0, h).start()

    y_copy(BACK, me, h_back.at[other]).start()

    def spread_act(h):
        act_copy(0, h).wait_recv()
        act_copy(2, h).start()
        act_copy(1, h).start()

    spread_act(0)
    relay(LEAD, 2, other)
    relay(REST, 1, why)
    spread_act(1)
    relay(REST, 2, why)
    relay(REST, 1, other)

    def sent(p, row):
        owner = zed * WIDTH + row
        pl.when(can_up)(lambda: z_copy(p, owner, UP).wait_send())
        pl.when(can_down)(lambda: z_copy(p, owner, DOWN).wait_send())
        for s in (1, 2):
            low, high = (zed - s) * WIDTH + row, (zed + s) * WIDTH + row
            pl.when((zed >= s) & can_up)(lambda: z_copy(p, low, UP).wait_send())
            pl.when((zed + s <= last_z) & can_down)(lambda: z_copy(p, high, DOWN).wait_send())

    for p in firsts:
        sent(p, why)
        y_copy(p, me).wait_send()
        for s in (1, 2, 3):
            low, high = (zed - s) * WIDTH + why, (zed + s) * WIDTH + why
            pl.when(zed >= s)(lambda: y_copy(p, low).wait_send())
            pl.when(zed + s <= last_z)(lambda: y_copy(p, high).wait_send())
    for k in range(3):
        mx_copy(None, k).wait_send()
    for k in range(3):
        tp_copy(1, k).wait_send()

    for h in range(2):
        act_copy(2, h).wait_recv()
        act_copy(3, h).start()
    relay(REST, 2, other)
    arrived(BACK, beside)
    own(BACK).wait()
    for row in range(WIDTH):
        z_own(BACK, row, None)
    for p in (LEAD, REST):
        own(p).wait()
    for row in (why, other):
        for s in (1, 2, 3):
            settle(LEAD, s, row)
    for h in range(2):
        act_copy(1, h).wait_recv()
        act_copy(3, h).wait_recv()

    def activate(weights, row_scales, first, write):
        @pl.loop(0, tiles)
        def _(i):
            rows = pl.ds(pl.multiple_of(first + i * ROWS, ROWS), ROWS)
            both = jnp.dot(act[rows, :], weights[...], preferred_element_type=f32)
            write(rows, both * row_scales[pl.ds(why, 1), :])

    def gate_with(gate, up):
        return gate / (1.0 + jnp.exp(-gate)) * up

    def write_lead(rows, both):
        hidden[rows, :cut] = gate_with(both[:, :cut], both[:, cut:]).astype(bf16)

    def write_rest(rows, both):
        tail = main - cut
        hidden[rows, cut:main] = gate_with(both[:, :tail], both[:, tail + 128 :]).astype(bf16)
        mixed_lanes = both[:, tail : tail + 128]
        ends = gate_with(mixed_lanes, pltpu.roll(mixed_lanes, 64, 1))
        lane = lax.broadcasted_iota(jnp.int32, ends.shape, 1)
        hidden[rows, main:] = jnp.where(lane < 64, ends, 0.0).astype(bf16)

    for half in (other, why):
        activate(lead, s_lead, half * count, write_lead)
    for row in (why, other):
        for s in (1, 2, 3):
            settle(REST, s, row)

    pieces = count // PIECE

    def piece(t):
        return pl.ds(pl.multiple_of(t * PIECE, PIECE), PIECE)

    def block_at(k):
        return lax.rem(zed + k * (1 - 2 * lax.div(zed, last_z)) + DEPTH, DEPTH)

    def core_copy(j, row, t):
        line = lax.div(j, 2)
        return pltpu.make_async_remote_copy(
            src_ref=part.at[j, row, piece(t), :],
            dst_ref=from_core.at[line, row, piece(t), :],
            send_sem=core_send.at[line, row],
            recv_sem=core_recv.at[line, row, t],
            device_id={"tp": sibling},
            device_id_type=MESH,
        )

    def sum_copy(j, row, q):
        line = lax.div(j, 2)
        return pltpu.make_async_remote_copy(
            src_ref=part.at[j, row, piece(other * pieces + q), :],
            dst_ref=from_y.at[line, row, piece(q), :],
            send_sem=sum_send.at[line, row, q],
            recv_sem=sum_recv.at[line, row, q],
            device_id={"fs": beside},
            device_id_type=MESH,
        )

    def last_copy(j, row, q):
        return pltpu.make_async_remote_copy(
            src_ref=part.at[j, row, piece(why * pieces + q), :],
            dst_ref=from_x.at[row, piece(q), :],
            send_sem=last_send.at[row, q],
            recv_sem=last_recv.at[row, q],
            device_id={"tp": across},
            device_id_type=MESH,
        )

    def multiply(k, row, half):
        j = block_at(k)
        wide = h_back.shape[2]
        columns = pl.ds(pl.multiple_of((j * WIDTH + row) * wide, wide), wide)

        @pl.loop(0, pieces)
        def _(q):
            t = half * pieces + q
            term = jnp.dot(hidden[piece(t), :], back[:, columns], preferred_element_type=f32)
            part[j, row, piece(t), :] = (term * scales[8:9, columns]).astype(bf16)
            pl.when(core != lax.rem(j, 2))(lambda: core_copy(j, row, t).start())

    def added(j, row, t, extra):
        return part[j, row, piece(t), :].astype(f32) + extra.astype(f32)

    def stage_1(k, row, half):
        j = block_at(k)

        @pl.when(core == lax.rem(j, 2))
        def _():
            line = lax.div(j, 2)
            for q in range(pieces):
                t = half * pieces + q
                core_copy(j, row, t).wait_recv()
                total = added(j, row, t, from_core[line, row, piece(t), :])
                part[j, row, piece(t), :] = total.astype(bf16)
                if half is other:
                    sum_copy(j, row, q).start()

    def stage_2(k, row):
        j = block_at(k)

        @pl.when(core == lax.rem(j, 2))
        def _():
            line = lax.div(j, 2)
            for q in range(pieces):
                t = why * pieces + q
                sum_copy(j, row, q).wait_recv()
                total = added(j, row, t, from_y[line, row, piece(q), :])
                part[j, row, piece(t), :] = total.astype(bf16)
                pl.when(ex != line)(lambda: last_copy(j, row, q).start())

    def stage_3(k, row):
        j = block_at(k)
        wide = h_back.shape[2]

        @pl.when(tp == j)
        def _():
            columns = pl.ds(row * wide, wide)
            for q in range(pieces):
                t = why * pieces + q
                last_copy(j, row, q).wait_recv()
                kept = residual_own[piece(q), columns].astype(f32)
                total = added(j, row, t, from_x[row, piece(q), :])
                out[piece(q), columns] = (kept + total).astype(bf16)

    activate(rest, s_rest, other * count, write_rest)
    for row in range(WIDTH):
        relay(BACK, 1, row)
    for row in range(WIDTH):
        multiply(0, row, other)
        stage_1(0, row, other)
    activate(rest, s_rest, base, write_rest)
    for row in range(WIDTH):
        multiply(0, row, why)
        stage_1(0, row, why)

    order = [(k, row) for k in range(DEPTH) for row in range(WIDTH)]
    after_unit = {
        3: ((stage_2, 0), (stage_2, 1)),
        4: ((stage_2, 2),),
        5: ((stage_2, 3), (stage_2, 4)),
        6: ((stage_2, 5), (stage_3, 0), (stage_3, 1)),
        7: (
            (stage_2, 6), (stage_2, 7), (stage_3, 2), (stage_3, 3), (stage_3, 4), (stage_3, 5),
            (stage_3, 6), (stage_3, 7),
        ),
    }
    for u, (k, row) in enumerate(order):
        if u == 2 * WIDTH:
            for line in range(WIDTH):
                relay(BACK, 2, line)
        if k:
            owner = block_at(k) * WIDTH + row
            pl.when(outer)(lambda: arrived(BACK, owner))
            for half in (other, why):
                multiply(k, row, half)
                stage_1(k, row, half)
        for stage, unit in after_unit.get(u, ()):
            stage(*order[unit])

    for p in (LEAD, REST, BACK):
        y_copy(p, me).wait_send()
        for row in range(WIDTH):
            sent(p, row)
    for k in range(4):
        for h in range(2):
            act_copy(k, h).wait_send()
    for k, row in order:
        j = block_at(k)

        @pl.when(core != lax.rem(j, 2))
        def _():
            pltpu.make_async_remote_copy(
                src_ref=part.at[j, row],
                dst_ref=from_core.at[lax.div(j, 2), row],
                send_sem=core_send.at[lax.div(j, 2), row],
                recv_sem=core_recv.at[lax.div(j, 2), row, 0],
                device_id={"tp": sibling},
                device_id_type=MESH,
            ).wait_send()

        @pl.when(core == lax.rem(j, 2))
        def _():
            for q in range(pieces):
                sum_copy(j, row, q).wait_send()
                pl.when(ex != lax.div(j, 2))(lambda: last_copy(j, row, q).wait_send())


def fused_device(
    tokens,
    mixer_gain,
    ffn_gain,
    w_outer,
    w_inner,
    w_value,
    scale_outer,
    scale_inner,
    scale_value,
    conv_taps,
    w_mixout,
    scale_mixout,
    w_gate,
    w_upward,
    scale_gate,
    scale_upward,
    w_down,
    scale_down,
):
    bf16 = jnp.bfloat16
    count, feat = tokens.shape
    model = mixer_gain.shape[0]
    chan = w_outer.shape[1]
    units = w_gate.shape[1]
    cols = w_down.shape[1]
    half = units // 2
    padded = half // 128 * 128 + 128
    cut = half // 128 * 3 // 5 * 128
    vmem = pl.BlockSpec(memory_space=pltpu.VMEM)
    hbm = pl.BlockSpec(memory_space=pl.ANY)
    dma = pltpu.SemaphoreType.DMA
    owners = DEPTH * WIDTH
    return pl.pallas_call(
        block_kernel,
        out_shape=pltpu.VMEM((count, feat), bf16),
        in_specs=[hbm if k in (0, 3, 4, 5, 10, 12, 13, 16) else vmem for k in range(18)],
        out_specs=vmem,
        scratch_shapes=[
            pltpu.VMEM((16, cols), jnp.float32),
            pltpu.VMEM((w_outer.shape[0], 3 * chan), bf16),
            pltpu.VMEM(w_mixout.shape, bf16),
            pltpu.VMEM((2, w_gate.shape[0], 2 * cut), bf16),
            pltpu.VMEM((2, w_gate.shape[0], units - 2 * cut), bf16),
            pltpu.VMEM((2, half, cols), bf16),
            pltpu.VMEM((2, 2 * cut), jnp.float32),
            pltpu.VMEM((2, units - 2 * cut), jnp.float32),
            pltpu.VMEM(w_gate.shape, jnp.float32),
            pltpu.VMEM(w_upward.shape, jnp.float32),
            pltpu.VMEM(w_down.shape, jnp.float32),
            pltpu.VMEM((3, *w_outer.shape), jnp.float32),
            pltpu.VMEM(w_mixout.shape, jnp.float32),
            pltpu.VMEM((2, 8, units), jnp.float32),
            pltpu.VMEM((WIDTH * count, model), bf16),
            pltpu.VMEM((model, 3 * chan), bf16),
            pltpu.VMEM((TP * chan, model), bf16),
            pltpu.VMEM((model, 2 * cut), bf16),
            pltpu.VMEM((model, units - 2 * cut), bf16),
            pltpu.VMEM((padded, model), bf16),
            pltpu.VMEM((16, model), jnp.float32),
            pltpu.VMEM((count, TP * chan), bf16),
            pltpu.VMEM((WIDTH * count, padded), bf16),
            pltpu.VMEM((count, feat), bf16),
            pltpu.VMEM((DEPTH, WIDTH, WIDTH * count, cols), bf16),
            pltpu.VMEM((2, WIDTH, WIDTH * count, cols), bf16),
            pltpu.VMEM((2, WIDTH, count, cols), bf16),
            pltpu.VMEM((WIDTH, count, cols), bf16),
            dma((9, DEPTH + 1)),
            dma((3 * DEPTH + 3,)),
            dma((6, owners)),
            dma((2, 3)),
            dma((2, 3)),
            dma((3,)),
            dma((owners,)),
            dma((2,)),
            dma((4, 2)),
            dma((4, 2)),
            dma((2, WIDTH)),
            dma((2, WIDTH, 4)),
            dma((2, WIDTH, 2)),
            dma((2, WIDTH, 2)),
            dma((WIDTH, 2)),
            dma((WIDTH, 2)),
            dma((14,)),
        ],
        compiler_params=pltpu.CompilerParams(
            collective_id=0, has_side_effects=True, vmem_limit_bytes=62 * 1024 * 1024
        ),
    )(
        tokens, mixer_gain[None], ffn_gain[None], w_outer, w_inner, w_value,
        scale_outer, scale_inner, scale_value, conv_taps, w_mixout, scale_mixout,
        w_gate, w_upward, scale_gate, scale_upward, w_down, scale_down,
    )


def plain_device(
    tokens,
    mixer_gain,
    ffn_gain,
    w_outer,
    w_inner,
    w_value,
    scale_outer,
    scale_inner,
    scale_value,
    conv_taps,
    w_mixout,
    scale_mixout,
    w_gate,
    w_upward,
    scale_gate,
    scale_upward,
    w_down,
    scale_down,
):
    full_rows = lax.all_gather(tokens, "tp", axis=1, tiled=True)
    normed = rms_scaled(full_rows, mixer_gain)
    tok_count = tokens.shape[0]
    local_channels = w_outer.shape[1]

    def add_one(w_piece):
        return add_rows(normed, w_piece)

    outer_bf = w_outer.astype(jnp.bfloat16)
    inner_bf = w_inner.astype(jnp.bfloat16)
    value_bf = w_value.astype(jnp.bfloat16)
    outer = add_one(lax.all_gather(outer_bf, "fs", axis=0, tiled=True))
    inner = add_one(lax.all_gather(inner_bf, "fs", axis=0, tiled=True))
    value = add_one(lax.all_gather(value_bf, "fs", axis=0, tiled=True))
    outer = outer * scale_outer
    product = inner * scale_inner * (value * scale_value)
    product = product.reshape(tok_count // SEQ_LEN, SEQ_LEN, local_channels)
    conv = causal_taps(product, conv_taps).reshape(tok_count, local_channels)
    mixed_out = (outer * conv).astype(jnp.bfloat16)
    mixout_scales, down_scales = (
        lax.all_gather(scale_mixout, "fs", axis=1, tiled=True),
        lax.all_gather(scale_down, "fs", axis=1, tiled=True),
    )
    mixout_bf = w_mixout.astype(jnp.bfloat16)
    mixed_all = lax.all_gather(mixed_out, "tp", axis=1, tiled=True)
    mixout_cols = lax.all_gather(mixout_bf, "fs", axis=1, tiled=True)
    mixout_all = lax.all_gather(mixout_cols, "tp", axis=0, tiled=True)
    mix_term = jnp.dot(mixed_all, mixout_all, preferred_element_type=jnp.float32) * mixout_scales
    residual_rows = (full_rows.astype(jnp.float32) + mix_term).astype(jnp.bfloat16)
    feature_count = tokens.shape[1]
    residual = lax.dynamic_slice_in_dim(
        residual_rows, lax.axis_index("tp") * feature_count, feature_count, 1
    )
    normed_ffn = rms_scaled(residual_rows, ffn_gain)
    gate_proj = add_rows(
        normed_ffn, lax.all_gather(w_gate.astype(jnp.bfloat16), "fs", axis=0, tiled=True)
    )
    up_proj = add_rows(
        normed_ffn, lax.all_gather(w_upward.astype(jnp.bfloat16), "fs", axis=0, tiled=True)
    )
    hidden = (jax.nn.silu(gate_proj * scale_gate) * (up_proj * scale_upward)).astype(jnp.bfloat16)
    down_terms = (
        jnp.dot(
            hidden,
            lax.all_gather(w_down.astype(jnp.bfloat16), "fs", axis=1, tiled=True),
            preferred_element_type=jnp.float32,
        )
        * down_scales
    )
    ffn_share = lax.psum_scatter(
        down_terms.astype(jnp.bfloat16), "tp", scatter_dimension=1, tiled=True
    ).astype(jnp.float32)
    return (residual.astype(jnp.float32) + ffn_share).astype(jnp.bfloat16)


def solution(mesh):
    in_specs = (
        P("fs", "tp"),
        P(),
        P(),
        P("fs", "tp"),
        P("fs", "tp"),
        P("fs", "tp"),
        P(None, "tp"),
        P(None, "tp"),
        P(None, "tp"),
        P(None, "tp"),
        P("tp", "fs"),
        P(None, "fs"),
        P("fs", "tp"),
        P("fs", "tp"),
        P(None, "tp"),
        P(None, "tp"),
        P("tp", "fs"),
        P(None, "fs"),
    )
    out_specs = P("fs", "tp")
    chosen = fused_device if (mesh.shape["fs"], mesh.shape["tp"]) == (8, 4) else plain_device
    return jax.shard_map(
        chosen, mesh=mesh, in_specs=in_specs, out_specs=out_specs, check_vma=False
    )
```

```python
import jax
import jax.numpy as jnp
from jax import lax
from jax.experimental import pallas as pl
from jax.experimental.pallas import tpu as pltpu
from jax.sharding import PartitionSpec as P

SEQ_LEN = 128


def rms_scaled(full_rows, gain_vec):
    values = full_rows.astype(jnp.float32)
    inverse = lax.rsqrt(jnp.mean(values * values, axis=-1, keepdims=True) + 1e-06)
    return (values * inverse * gain_vec).astype(jnp.bfloat16)


def add_rows(left, w_piece):
    return jnp.dot(left, w_piece, preferred_element_type=jnp.float32)


def causal_taps(product, conv_taps):
    padded = jnp.pad(product, ((0, 0), (conv_taps.shape[0] - 1, 0), (0, 0)))
    length = product.shape[1]
    summed = jnp.zeros(product.shape, jnp.float32)
    for tap_index in range(conv_taps.shape[0]):
        summed = summed + conv_taps[tap_index] * padded[:, tap_index : tap_index + length, :]
    return summed


DEPTH, WIDTH, TP = 4, 2, 4
ROWS = 256
PIECE = 512
UP, DOWN = 0, 1
SCALES, MIXER, MIXOUT, LEAD, REST, BACK, BACK_END = range(7)
MESH = pl.DeviceIdType.MESH


def block_kernel(
    tokens, mixer_gain, ffn_gain, w_outer, w_inner, w_value, s_outer, s_inner, s_value, taps,
    w_mixout, s_mixout, w_gate, w_upward, s_gate, s_upward, w_down, s_down,
    out,
    h_scales, h_mixer, h_mixout, h_lead, h_rest, h_back, h_back_end, s_lead, s_rest, raw_gate, raw_up, raw_down,
    raw_mixer, raw_mixout, raw_scale,
    act, mixer, mixout, lead, rest, back, scales, mixed, hidden, residual_own,
    part, from_core, from_y, from_x,
    z_send, y_send, fs_recv, tp_send, tp_recv, mx_send, mx_recv, mx_whole,
    act_send, act_recv, core_send, core_recv, sum_send, sum_recv, last_send, last_recv,
    local_sem,
):
    f32, bf16 = jnp.float32, jnp.bfloat16
    me, tp = lax.axis_index("fs"), lax.axis_index("tp")
    zed, why = lax.div(me, WIDTH), lax.rem(me, WIDTH)
    ex, core = lax.div(tp, 2), lax.rem(tp, 2)
    other = 1 - why
    last_z = DEPTH - 1
    count = tokens.shape[0]
    tiles = count // ROWS

    beside = zed * WIDTH + other
    sibling = ex * 2 + (1 - core)
    across = (1 - ex) * 2 + core

    wide = w_outer.shape[1]
    fetched = (
        (w_outer, raw_mixer.at[0]), (w_inner, raw_mixer.at[1]), (w_value, raw_mixer.at[2]),
        (w_mixout, raw_mixout), (w_gate, raw_gate), (w_upward, raw_up), (w_down, raw_down),
    )

    def fetch(k):
        return pltpu.make_async_copy(*fetched[k], local_sem.at[8 + k])

    for k in range(len(fetched)):
        fetch(k).start()
    barrier = pltpu.get_barrier_semaphore()
    ring = [lax.rem(zed + step, DEPTH) * WIDTH + why for step in (1, DEPTH - 1)]
    for peer in (beside, *ring):
        pl.semaphore_signal(barrier, inc=1, device_id={"fs": peer}, device_id_type=MESH)
    for peer in (sibling, across):
        pl.semaphore_signal(barrier, inc=1, device_id={"tp": peer}, device_id_type=MESH)
    for k in range(4):
        fetch(k).wait()
    for k in range(3):
        h_mixer[:, k * wide : (k + 1) * wide] = raw_mixer[k].astype(bf16)
    h_mixout[...] = raw_mixout[...].astype(bf16)
    for k, row in enumerate((s_mixout, s_down)):
        h_scales[k * 4 : (k + 1) * 4, :] = jnp.broadcast_to(row[...], (4, row.shape[1]))
    pl.semaphore_wait(barrier, 5)

    fulls = (scales, mixer, mixout, lead, rest, back, back)
    split = (h_lead, h_rest, h_back, h_back_end)
    own_src = (h_scales, h_mixer, h_mixout, *[h.at[why] for h in split])

    def place(p, owner):
        if p in (MIXER, LEAD, REST):
            height = own_src[p].shape[0]
            return fulls[p].at[pl.ds(pl.multiple_of(owner * height, height), height), :]
        height, wide = own_src[p].shape
        first = pl.multiple_of(tp * height, height) if p == MIXOUT else 0
        start = owner * wide
        if p >= BACK:
            start = owner * 2 * wide + (p - BACK) * wide
        return fulls[p].at[pl.ds(first, height), pl.ds(pl.multiple_of(start, wide), wide)]

    first_own = LEAD * DEPTH - LEAD

    def kind(p, owner):
        return p if p < LEAD else LEAD + (p - LEAD) * WIDTH + lax.rem(owner, WIDTH)

    def line_of(owner, way):
        z = lax.div(owner, WIDTH)
        return z if way == UP else lax.select(z == zed, DEPTH, z)

    def z_copy(p, owner, way, src=None):
        spot = place(p, owner)
        step = 1 if way == UP else -1
        return pltpu.make_async_remote_copy(
            src_ref=spot if src is None else src,
            dst_ref=spot,
            send_sem=z_send.at[kind(p, owner), line_of(owner, way)],
            recv_sem=fs_recv.at[p, owner],
            device_id={"fs": (zed + step) * WIDTH + why},
            device_id_type=MESH,
        )

    def y_copy(p, owner, src=None):
        spot = place(p, owner)
        return pltpu.make_async_remote_copy(
            src_ref=spot if src is None else src,
            dst_ref=spot,
            send_sem=y_send.at[p * DEPTH + lax.div(owner, WIDTH) if p < LEAD else first_own + p],
            recv_sem=fs_recv.at[p, owner],
            device_id={"fs": beside},
            device_id_type=MESH,
        )

    def arrived(p, owner):
        y_copy(p, owner).wait_recv()

    def own(p):
        return pltpu.make_async_copy(own_src[p], place(p, me), local_sem.at[p])

    can_up, can_down = zed < last_z, zed > 0
    outer = (zed == 0) | (zed == last_z)

    def z_own(p, row, src):
        owner = zed * WIDTH + row
        pl.when(can_up)(lambda: z_copy(p, owner, UP, src).start())
        pl.when(can_down)(lambda: z_copy(p, owner, DOWN, src).start())

    def relay(p, s, row):
        low, high = (zed - s) * WIDTH + row, (zed + s) * WIDTH + row

        @pl.when((zed >= s) & can_up)
        def _():
            arrived(p, low)
            z_copy(p, low, UP).start()

        @pl.when((zed + s <= last_z) & can_down)
        def _():
            arrived(p, high)
            z_copy(p, high, DOWN).start()

    def settle(p, s, row):
        low, high = (zed - s) * WIDTH + row, (zed + s) * WIDTH + row
        pl.when((zed >= s) & (zed == last_z))(lambda: arrived(p, low))
        pl.when((zed + s <= last_z) & (zed == 0))(lambda: arrived(p, high))

    def mx_copy(owner, k, src=None):
        line, target = ((tp, sibling), (tp, across), (across, sibling))[k]
        height, wide = h_mixout.shape
        columns = slice(None)
        if owner is not None:
            columns = pl.ds(pl.multiple_of(owner * wide, wide), wide)
        spot = mixout.at[pl.ds(pl.multiple_of(line * height, height), height), columns]
        return pltpu.make_async_remote_copy(
            src_ref=spot if src is None else src,
            dst_ref=spot,
            send_sem=mx_send.at[k],
            recv_sem=mx_recv.at[0 if owner is None else owner] if k == 1 else mx_whole.at[k // 2],
            device_id={"tp": target},
            device_id_type=MESH,
        )

    def mx_first(owner, src=None):
        mx_copy(owner, 1, src).start()
        mx_copy(owner, 0, src).start()

    firsts = (SCALES, MIXOUT, MIXER)

    def relay_first(s):
        low, high = (zed - s) * WIDTH + why, (zed + s) * WIDTH + why

        @pl.when(zed >= s)
        def _():
            for p in firsts:
                arrived(p, low)
                pl.when(can_up)(lambda: z_copy(p, low, UP).start())
                y_copy(p, low).start()
                if p == MIXOUT:
                    mx_first(low)

        @pl.when(zed + s <= last_z)
        def _():
            for p in firsts:
                arrived(p, high)
                pl.when(can_down)(lambda: z_copy(p, high, DOWN).start())
                y_copy(p, high).start()
                if p == MIXOUT:
                    mx_first(high)

    def from_beside(s):
        def take(owner):
            for p in firsts:
                arrived(p, owner)
                if p == MIXOUT:
                    mx_first(owner)

        if s == 0:
            take(beside)
            return
        low, high = (zed - s) * WIDTH + other, (zed + s) * WIDTH + other
        pl.when(zed >= s)(lambda: take(low))
        pl.when(zed + s <= last_z)(lambda: take(high))

    base = pl.multiple_of(why * count, count)

    def tp_slot(a, owner):
        if a == 0:
            wide = tokens.shape[1]
            return act.at[pl.ds(base, count), pl.ds(pl.multiple_of(owner * wide, wide), wide)]
        wide = mixed.shape[1] // TP
        return mixed.at[:, pl.ds(pl.multiple_of(owner * wide, wide), wide)]

    def tp_copy(a, k):
        owner, target = ((tp, sibling), (tp, across), (across, sibling))[k]
        spot = tp_slot(a, owner)
        return pltpu.make_async_remote_copy(
            src_ref=tokens if a == 0 and k < 2 else spot,
            dst_ref=spot,
            send_sem=tp_send.at[a, k],
            recv_sem=tp_recv.at[a, k],
            device_id={"tp": target},
            device_id_type=MESH,
        )

    def tp_first(a):
        tp_copy(a, 1).start()
        tp_copy(a, 0).start()

    def tp_second(a):
        tp_copy(a, 1).wait_recv()
        tp_copy(a, 2).start()

    def tp_finish(a):
        tp_copy(a, 0).wait_recv()
        tp_copy(a, 2).wait_recv()

    own_tokens = pltpu.make_async_copy(tokens, tp_slot(0, tp), local_sem.at[7])

    for p in firsts:
        y_copy(p, me, own_src[p]).start()
        z_own(p, why, own_src[p])
    tp_first(0)
    mx_first(me, h_mixout)
    own_tokens.start()
    for p in firsts:
        own(p).start()
    units = h_back.shape[1]
    main = units // 128 * 128
    middle, after = pl.ds(main, 128), main + 128

    cut = h_lead.shape[2] // 2

    def share_out(gate, up, write):
        tail = main - cut
        for half, first in enumerate((0, after)):
            for k, source in enumerate((gate, up)):
                write(0, half, pl.ds(k * cut, cut), source[:, pl.ds(first, cut)])
                at = pl.ds(k * (tail + 128), tail)
                write(1, half, at, source[:, pl.ds(first + cut, tail)])
        gate, up = gate[:, middle], up[:, middle]
        low = lax.broadcasted_iota(jnp.int32, gate.shape, 1) < 64
        write(1, 0, pl.ds(tail, 128), jnp.where(low, gate, pltpu.roll(up, 64, 1)))
        write(1, 1, pl.ds(tail, 128), jnp.where(low, pltpu.roll(gate, 64, 1), up))

    def write_scale(target, half, lanes, values):
        (s_lead, s_rest)[target][half : half + 1, lanes] = values[0:1]

    def write_gated(target, half, lanes, values):
        split[target][half, :, lanes] = values.astype(bf16)

    for k in range(4, len(fetched)):
        fetch(k).wait()
    share_out(raw_gate, raw_up, write_gated)
    narrow = h_back.shape[2]
    for k, target in enumerate((h_back, h_back_end)):
        lanes = pl.ds(k * narrow, narrow)
        target[0] = raw_down[:units, lanes].astype(bf16)
        target[1, :main, :] = raw_down[after:, lanes].astype(bf16)
        target[1, main:, :] = raw_down[units:after, lanes].astype(bf16)
    for k, row in enumerate((s_gate, s_upward)):
        raw_scale[k] = jnp.broadcast_to(row[...], raw_scale.shape[1:])
    share_out(raw_scale.at[0], raw_scale.at[1], write_scale)
    for p in (LEAD, REST, BACK, BACK_END):
        own(p).start()
    back[units:, :] = jnp.zeros((back.shape[0] - units, back.shape[1]), bf16)

    @pl.when(outer)
    def _():
        for p in (LEAD, REST):
            z_own(p, why, own_src[p])

    relay_first(1)
    tp_second(0)
    relay_first(2)
    pl.when(jnp.logical_not(outer))(lambda: z_own(LEAD, why, own_src[LEAD]))
    relay_first(3)
    y_copy(LEAD, me, h_lead.at[other]).start()
    y_copy(REST, me, h_rest.at[other]).start()
    relay(LEAD, 1, why)
    for s in range(DEPTH):
        from_beside(s)
    relay(LEAD, 2, why)
    tp_finish(0)
    own_tokens.wait()
    for p in firsts:
        own(p).wait()

    chan = mixed.shape[1] // TP

    def tile(i):
        return pl.ds(pl.multiple_of(i * ROWS, ROWS), ROWS)

    def own_rows(i):
        return pl.ds(pl.multiple_of(base + i * ROWS, ROWS), ROWS)

    def normalised(values, gain):
        inverse = lax.rsqrt(jnp.mean(values * values, axis=-1, keepdims=True) + 1e-06)
        return (values * inverse * gain[...]).astype(bf16)

    @pl.loop(0, tiles)
    def _(i):
        normed = normalised(act[own_rows(i), :].astype(f32), mixer_gain)
        three = jnp.dot(normed, mixer[...], preferred_element_type=f32)
        product = (three[:, chan : 2 * chan] * s_inner[...]) * (three[:, 2 * chan :] * s_value[...])
        row = lax.rem(lax.broadcasted_iota(jnp.int32, product.shape, 0), SEQ_LEN)
        total = jnp.zeros_like(product)
        last = taps.shape[0] - 1
        for j in range(taps.shape[0]):
            gap = last - j
            moved = product
            if gap:
                moved = jnp.where(row >= gap, pltpu.roll(product, gap, 0), 0.0)
            total = total + taps[j : j + 1, :] * moved
        mixed[tile(i), pl.ds(pl.multiple_of(tp * chan, chan), chan)] = (
            three[:, :chan] * s_outer[...] * total
        ).astype(bf16)

    tp_first(1)
    arrived(LEAD, beside)
    z_own(LEAD, other, None)
    pl.when(jnp.logical_not(outer))(lambda: z_own(REST, why, own_src[REST]))
    for owner in range(DEPTH * WIDTH):
        mx_copy(owner, 1).wait_recv()
        mx_copy(owner, 2).start()
    tp_second(1)
    relay(LEAD, 1, other)
    mx_copy(None, 0).wait_recv()
    mx_copy(None, 2).wait_recv()
    tp_finish(1)
    for k in range(3):
        tp_copy(0, k).wait_send()

    arrived(REST, beside)
    z_own(REST, other, None)

    feat = tokens.shape[1]
    quarter = count // TP
    strip = quarter // 2

    def act_copy(k, h):
        half, owner, target = (
            (why, tp, {"fs": beside}),
            (other, tp, {"tp": sibling}),
            (other, tp, {"tp": across}),
            (other, across, {"tp": sibling}),
        )[k]
        first = half * count + owner * quarter + h * strip
        spot = act.at[pl.ds(pl.multiple_of(first, strip), strip), :]
        return pltpu.make_async_remote_copy(
            src_ref=spot,
            dst_ref=spot,
            send_sem=act_send.at[k, h],
            recv_sem=act_recv.at[k, h],
            device_id=target,
            device_id_type=MESH,
        )

    @pl.loop(0, tiles)
    def _(step):
        i = lax.rem(step + tp, tiles)
        term = jnp.dot(mixed[tile(i), :], mixout[...], preferred_element_type=f32)
        term = term * scales[0:1, :]
        residual = (act[own_rows(i), :].astype(f32) + term).astype(bf16)
        act[own_rows(i), :] = residual
        residual_own[tile(i), :] = act[
            own_rows(i), pl.ds(pl.multiple_of(tp * feat, feat), feat)
        ]
        act[own_rows(i), :] = normalised(residual.astype(f32), ffn_gain)

        @pl.when(step == 0)
        def _():
            for h in range(2):
                act_copy(0, h).start()

    y_copy(BACK, me, h_back.at[other]).start()
    y_copy(BACK_END, me, h_back_end.at[other]).start()

    def spread_act(h):
        act_copy(0, h).wait_recv()
        act_copy(2, h).start()
        act_copy(1, h).start()

    spread_act(0)
    relay(LEAD, 2, other)
    relay(REST, 1, why)
    spread_act(1)
    relay(REST, 2, why)
    relay(REST, 1, other)

    def sent(p, row):
        owner = zed * WIDTH + row
        pl.when(can_up)(lambda: z_copy(p, owner, UP).wait_send())
        pl.when(can_down)(lambda: z_copy(p, owner, DOWN).wait_send())
        for s in (1, 2):
            low, high = (zed - s) * WIDTH + row, (zed + s) * WIDTH + row
            pl.when((zed >= s) & can_up)(lambda: z_copy(p, low, UP).wait_send())
            pl.when((zed + s <= last_z) & can_down)(lambda: z_copy(p, high, DOWN).wait_send())

    for p in firsts:
        sent(p, why)
        y_copy(p, me).wait_send()
        for s in (1, 2, 3):
            low, high = (zed - s) * WIDTH + why, (zed + s) * WIDTH + why
            pl.when(zed >= s)(lambda: y_copy(p, low).wait_send())
            pl.when(zed + s <= last_z)(lambda: y_copy(p, high).wait_send())
    for k in range(3):
        mx_copy(None, k).wait_send()
    for k in range(3):
        tp_copy(1, k).wait_send()

    for h in range(2):
        act_copy(2, h).wait_recv()
        act_copy(3, h).start()
    relay(REST, 2, other)
    for p in (BACK, BACK_END):
        arrived(p, beside)
        own(p).wait()
    for row in range(WIDTH):
        for p in (BACK, BACK_END):
            z_own(p, row, None)
    for p in (LEAD, REST):
        own(p).wait()
    for row in (why, other):
        for s in (1, 2, 3):
            settle(LEAD, s, row)
    for h in range(2):
        act_copy(1, h).wait_recv()
        act_copy(3, h).wait_recv()

    def activate(weights, row_scales, first, write):
        @pl.loop(0, tiles)
        def _(i):
            rows = pl.ds(pl.multiple_of(first + i * ROWS, ROWS), ROWS)
            both = jnp.dot(act[rows, :], weights[...], preferred_element_type=f32)
            write(rows, both * row_scales[pl.ds(why, 1), :])

    def gate_with(gate, up):
        return gate / (1.0 + jnp.exp(-gate)) * up

    def write_lead(rows, both):
        hidden[rows, :cut] = gate_with(both[:, :cut], both[:, cut:]).astype(bf16)

    def write_rest(rows, both):
        tail = main - cut
        hidden[rows, cut:main] = gate_with(both[:, :tail], both[:, tail + 128 :]).astype(bf16)
        mixed_lanes = both[:, tail : tail + 128]
        ends = gate_with(mixed_lanes, pltpu.roll(mixed_lanes, 64, 1))
        lane = lax.broadcasted_iota(jnp.int32, ends.shape, 1)
        hidden[rows, main:] = jnp.where(lane < 64, ends, 0.0).astype(bf16)

    for half in (other, why):
        activate(lead, s_lead, half * count, write_lead)
    for row in (why, other):
        for s in (1, 2, 3):
            settle(REST, s, row)

    pieces = count // PIECE

    def piece(t):
        return pl.ds(pl.multiple_of(t * PIECE, PIECE), PIECE)

    def block_at(k):
        return lax.rem(zed + k * (1 - 2 * lax.div(zed, last_z)) + DEPTH, DEPTH)

    def region(ref, half, q, by_columns):
        if by_columns:
            wide = h_back.shape[2]
            return ref.at[pl.ds(pl.multiple_of(half * count, count), count), pl.ds(q * wide, wide)]
        return ref.at[piece(half * pieces + q), :]

    def core_copy(j, row, half, q, by_columns):
        line, t = lax.div(j, 2), half * pieces + q
        return pltpu.make_async_remote_copy(
            src_ref=region(part.at[j, row], half, q, by_columns),
            dst_ref=region(from_core.at[line, row], half, q, by_columns),
            send_sem=core_send.at[line, row],
            recv_sem=core_recv.at[line, row, t],
            device_id={"tp": sibling},
            device_id_type=MESH,
        )

    def sum_copy(j, row, q, by_columns):
        line = lax.div(j, 2)
        return pltpu.make_async_remote_copy(
            src_ref=region(part.at[j, row], other, q, by_columns),
            dst_ref=region(from_y.at[line, row], 0, q, by_columns),
            send_sem=sum_send.at[line, row, q],
            recv_sem=sum_recv.at[line, row, q],
            device_id={"fs": beside},
            device_id_type=MESH,
        )

    def last_copy(j, row, q, by_columns):
        return pltpu.make_async_remote_copy(
            src_ref=region(part.at[j, row], why, q, by_columns),
            dst_ref=region(from_x.at[row], 0, q, by_columns),
            send_sem=last_send.at[row, q],
            recv_sem=last_recv.at[row, q],
            device_id={"tp": across},
            device_id_type=MESH,
        )

    def is_last(k, row):
        return k == last_z and row == WIDTH - 1

    def multiply(k, row, half):
        j = block_at(k)
        wide = 2 * h_back.shape[2]
        columns = pl.ds(pl.multiple_of((j * WIDTH + row) * wide, wide), wide)

        @pl.loop(0, pieces)
        def _(q):
            t = half * pieces + q
            term = jnp.dot(hidden[piece(t), :], back[:, columns], preferred_element_type=f32)
            part[j, row, piece(t), :] = (term * scales[4:5, columns]).astype(bf16)
            pl.when(core != lax.rem(j, 2))(lambda: core_copy(j, row, half, q, False).start())

    def multiply_narrow(k, row, half, q):
        j = block_at(k)
        wide = h_back.shape[2]
        start = (j * WIDTH + row) * 2 * wide + q * wide
        columns = pl.ds(pl.multiple_of(start, wide), wide)

        @pl.loop(0, pieces)
        def _(i):
            t = half * pieces + i
            term = jnp.dot(hidden[piece(t), :], back[:, columns], preferred_element_type=f32)
            part[j, row, piece(t), pl.ds(q * wide, wide)] = (
                term * scales[4:5, columns]
            ).astype(bf16)

        pl.when(core != lax.rem(j, 2))(lambda: core_copy(j, row, half, q, True).start())

    def added(j, row, half, q, by_columns, extra):
        spot = region(part.at[j, row], half, q, by_columns)
        return spot[...].astype(f32) + extra[...].astype(f32)

    def stage_1(k, row, half, some=None):
        j, by = block_at(k), is_last(k, row)

        @pl.when(core == lax.rem(j, 2))
        def _():
            line = lax.div(j, 2)
            for q in range(pieces) if some is None else (some,):
                core_copy(j, row, half, q, by).wait_recv()
                extra = region(from_core.at[line, row], half, q, by)
                total = added(j, row, half, q, by, extra)
                region(part.at[j, row], half, q, by)[...] = total.astype(bf16)
                if half is other:
                    sum_copy(j, row, q, by).start()

    def stage_2(k, row, some=None):
        j, by = block_at(k), is_last(k, row)

        @pl.when(core == lax.rem(j, 2))
        def _():
            line = lax.div(j, 2)
            for q in range(pieces) if some is None else (some,):
                sum_copy(j, row, q, by).wait_recv()
                total = added(j, row, why, q, by, region(from_y.at[line, row], 0, q, by))
                region(part.at[j, row], why, q, by)[...] = total.astype(bf16)
                pl.when(ex != line)(lambda: last_copy(j, row, q, by).start())

    def stage_3(k, row):
        j, by = block_at(k), is_last(k, row)
        wide = 2 * h_back.shape[2]

        @pl.when(tp == j)
        def _():
            for q in range(pieces):
                last_copy(j, row, q, by).wait_recv()
                total = added(j, row, why, q, by, region(from_x.at[row], 0, q, by))
                lanes = pl.ds(row * wide, wide)
                kept = region(residual_own.at[:, lanes], 0, q, by)[...].astype(f32)
                region(out.at[:, lanes], 0, q, by)[...] = (kept + total).astype(bf16)

    activate(rest, s_rest, other * count, write_rest)
    for row in range(WIDTH):
        for p in (BACK, BACK_END):
            relay(p, 1, row)
    for row in range(WIDTH):
        multiply(0, row, other)
        stage_1(0, row, other)
    activate(rest, s_rest, base, write_rest)
    for row in range(WIDTH):
        multiply(0, row, why)
        stage_1(0, row, why)

    order = [(k, row) for k in range(DEPTH) for row in range(WIDTH)]
    after_unit = {
        3: ((stage_2, 0), (stage_2, 1)),
        4: ((stage_2, 2),),
        5: ((stage_2, 3), (stage_2, 4)),
        6: ((stage_2, 5), (stage_3, 0), (stage_3, 1)),
        7: (
            (stage_2, 7), (stage_3, 2), (stage_3, 3), (stage_3, 4), (stage_3, 5),
            (stage_3, 6), (stage_3, 7),
        ),
    }
    for u, (k, row) in enumerate(order):
        if u == 2 * WIDTH:
            for line in range(WIDTH):
                for p in (BACK, BACK_END):
                    relay(p, 2, line)
        if k:
            owner = block_at(k) * WIDTH + row
            if is_last(k, row):
                for q in range(pieces):
                    pl.when(outer)(lambda: arrived(BACK + q, owner))
                    for half in (other, why):
                        multiply_narrow(k, row, half, q)
                        stage_1(k, row, half, q)
                    stage_2(*order[u - 1], q)
            else:
                for p in (BACK, BACK_END):
                    pl.when(outer)(lambda: arrived(p, owner))
                for half in (other, why):
                    multiply(k, row, half)
                    stage_1(k, row, half)
        for stage, unit in after_unit.get(u, ()):
            stage(*order[unit])

    for p in (LEAD, REST, BACK, BACK_END):
        y_copy(p, me).wait_send()
        for row in range(WIDTH):
            sent(p, row)
    for k in range(4):
        for h in range(2):
            act_copy(k, h).wait_send()
    for k, row in order:
        j = block_at(k)

        @pl.when(core != lax.rem(j, 2))
        def _():
            pltpu.make_async_remote_copy(
                src_ref=part.at[j, row],
                dst_ref=from_core.at[lax.div(j, 2), row],
                send_sem=core_send.at[lax.div(j, 2), row],
                recv_sem=core_recv.at[lax.div(j, 2), row, 0],
                device_id={"tp": sibling},
                device_id_type=MESH,
            ).wait_send()

        @pl.when(core == lax.rem(j, 2))
        def _():
            for q in range(pieces):
                by = is_last(k, row)
                sum_copy(j, row, q, by).wait_send()
                pl.when(ex != lax.div(j, 2))(lambda: last_copy(j, row, q, by).wait_send())


def fused_device(
    tokens,
    mixer_gain,
    ffn_gain,
    w_outer,
    w_inner,
    w_value,
    scale_outer,
    scale_inner,
    scale_value,
    conv_taps,
    w_mixout,
    scale_mixout,
    w_gate,
    w_upward,
    scale_gate,
    scale_upward,
    w_down,
    scale_down,
):
    bf16 = jnp.bfloat16
    count, feat = tokens.shape
    model = mixer_gain.shape[0]
    chan = w_outer.shape[1]
    units = w_gate.shape[1]
    cols = w_down.shape[1]
    half = units // 2
    padded = half // 128 * 128 + 128
    cut = half // 128 * 4 // 5 * 128
    vmem = pl.BlockSpec(memory_space=pltpu.VMEM)
    hbm = pl.BlockSpec(memory_space=pl.ANY)
    dma = pltpu.SemaphoreType.DMA
    owners = DEPTH * WIDTH
    return pl.pallas_call(
        block_kernel,
        out_shape=pltpu.VMEM((count, feat), bf16),
        in_specs=[hbm if k in (0, 3, 4, 5, 10, 12, 13, 16) else vmem for k in range(18)],
        out_specs=vmem,
        scratch_shapes=[
            pltpu.VMEM((8, cols), jnp.float32),
            pltpu.VMEM((w_outer.shape[0], 3 * chan), bf16),
            pltpu.VMEM(w_mixout.shape, bf16),
            pltpu.VMEM((2, w_gate.shape[0], 2 * cut), bf16),
            pltpu.VMEM((2, w_gate.shape[0], units - 2 * cut), bf16),
            pltpu.VMEM((2, half, cols // 2), bf16),
            pltpu.VMEM((2, half, cols // 2), bf16),
            pltpu.VMEM((2, 2 * cut), jnp.float32),
            pltpu.VMEM((2, units - 2 * cut), jnp.float32),
            pltpu.VMEM(w_gate.shape, jnp.float32),
            pltpu.VMEM(w_upward.shape, jnp.float32),
            pltpu.VMEM(w_down.shape, jnp.float32),
            pltpu.VMEM((3, *w_outer.shape), jnp.float32),
            pltpu.VMEM(w_mixout.shape, jnp.float32),
            pltpu.VMEM((2, 8, units), jnp.float32),
            pltpu.VMEM((WIDTH * count, model), bf16),
            pltpu.VMEM((model, 3 * chan), bf16),
            pltpu.VMEM((TP * chan, model), bf16),
            pltpu.VMEM((model, 2 * cut), bf16),
            pltpu.VMEM((model, units - 2 * cut), bf16),
            pltpu.VMEM((padded, model), bf16),
            pltpu.VMEM((8, model), jnp.float32),
            pltpu.VMEM((count, TP * chan), bf16),
            pltpu.VMEM((WIDTH * count, padded), bf16),
            pltpu.VMEM((count, feat), bf16),
            pltpu.VMEM((DEPTH, WIDTH, WIDTH * count, cols), bf16),
            pltpu.VMEM((2, WIDTH, WIDTH * count, cols), bf16),
            pltpu.VMEM((2, WIDTH, count, cols), bf16),
            pltpu.VMEM((WIDTH, count, cols), bf16),
            dma((11, DEPTH + 1)),
            dma((3 * DEPTH + 4,)),
            dma((7, owners)),
            dma((2, 3)),
            dma((2, 3)),
            dma((3,)),
            dma((owners,)),
            dma((2,)),
            dma((4, 2)),
            dma((4, 2)),
            dma((2, WIDTH)),
            dma((2, WIDTH, 4)),
            dma((2, WIDTH, 2)),
            dma((2, WIDTH, 2)),
            dma((WIDTH, 2)),
            dma((WIDTH, 2)),
            dma((15,)),
        ],
        compiler_params=pltpu.CompilerParams(
            collective_id=0, has_side_effects=True, vmem_limit_bytes=62 * 1024 * 1024
        ),
    )(
        tokens, mixer_gain[None], ffn_gain[None], w_outer, w_inner, w_value,
        scale_outer, scale_inner, scale_value, conv_taps, w_mixout, scale_mixout,
        w_gate, w_upward, scale_gate, scale_upward, w_down, scale_down,
    )


def plain_device(
    tokens,
    mixer_gain,
    ffn_gain,
    w_outer,
    w_inner,
    w_value,
    scale_outer,
    scale_inner,
    scale_value,
    conv_taps,
    w_mixout,
    scale_mixout,
    w_gate,
    w_upward,
    scale_gate,
    scale_upward,
    w_down,
    scale_down,
):
    full_rows = lax.all_gather(tokens, "tp", axis=1, tiled=True)
    normed = rms_scaled(full_rows, mixer_gain)
    tok_count = tokens.shape[0]
    local_channels = w_outer.shape[1]

    def add_one(w_piece):
        return add_rows(normed, w_piece)

    outer_bf = w_outer.astype(jnp.bfloat16)
    inner_bf = w_inner.astype(jnp.bfloat16)
    value_bf = w_value.astype(jnp.bfloat16)
    outer = add_one(lax.all_gather(outer_bf, "fs", axis=0, tiled=True))
    inner = add_one(lax.all_gather(inner_bf, "fs", axis=0, tiled=True))
    value = add_one(lax.all_gather(value_bf, "fs", axis=0, tiled=True))
    outer = outer * scale_outer
    product = inner * scale_inner * (value * scale_value)
    product = product.reshape(tok_count // SEQ_LEN, SEQ_LEN, local_channels)
    conv = causal_taps(product, conv_taps).reshape(tok_count, local_channels)
    mixed_out = (outer * conv).astype(jnp.bfloat16)
    mixout_scales, down_scales = (
        lax.all_gather(scale_mixout, "fs", axis=1, tiled=True),
        lax.all_gather(scale_down, "fs", axis=1, tiled=True),
    )
    mixout_bf = w_mixout.astype(jnp.bfloat16)
    mixed_all = lax.all_gather(mixed_out, "tp", axis=1, tiled=True)
    mixout_cols = lax.all_gather(mixout_bf, "fs", axis=1, tiled=True)
    mixout_all = lax.all_gather(mixout_cols, "tp", axis=0, tiled=True)
    mix_term = jnp.dot(mixed_all, mixout_all, preferred_element_type=jnp.float32) * mixout_scales
    residual_rows = (full_rows.astype(jnp.float32) + mix_term).astype(jnp.bfloat16)
    feature_count = tokens.shape[1]
    residual = lax.dynamic_slice_in_dim(
        residual_rows, lax.axis_index("tp") * feature_count, feature_count, 1
    )
    normed_ffn = rms_scaled(residual_rows, ffn_gain)
    gate_proj = add_rows(
        normed_ffn, lax.all_gather(w_gate.astype(jnp.bfloat16), "fs", axis=0, tiled=True)
    )
    up_proj = add_rows(
        normed_ffn, lax.all_gather(w_upward.astype(jnp.bfloat16), "fs", axis=0, tiled=True)
    )
    hidden = (jax.nn.silu(gate_proj * scale_gate) * (up_proj * scale_upward)).astype(jnp.bfloat16)
    down_terms = (
        jnp.dot(
            hidden,
            lax.all_gather(w_down.astype(jnp.bfloat16), "fs", axis=1, tiled=True),
            preferred_element_type=jnp.float32,
        )
        * down_scales
    )
    ffn_share = lax.psum_scatter(
        down_terms.astype(jnp.bfloat16), "tp", scatter_dimension=1, tiled=True
    ).astype(jnp.float32)
    return (residual.astype(jnp.float32) + ffn_share).astype(jnp.bfloat16)


def solution(mesh):
    in_specs = (
        P("fs", "tp"),
        P(),
        P(),
        P("fs", "tp"),
        P("fs", "tp"),
        P("fs", "tp"),
        P(None, "tp"),
        P(None, "tp"),
        P(None, "tp"),
        P(None, "tp"),
        P("tp", "fs"),
        P(None, "fs"),
        P("fs", "tp"),
        P("fs", "tp"),
        P(None, "tp"),
        P(None, "tp"),
        P("tp", "fs"),
        P(None, "fs"),
    )
    out_specs = P("fs", "tp")
    chosen = fused_device if (mesh.shape["fs"], mesh.shape["tp"]) == (8, 4) else plain_device
    return jax.shard_map(
        chosen, mesh=mesh, in_specs=in_specs, out_specs=out_specs, check_vma=False
    )
```

```python
import jax
import jax.numpy as jnp
from jax import lax
from jax.experimental import pallas as pl
from jax.experimental.pallas import tpu as pltpu
from jax.sharding import PartitionSpec as P

SEQ_LEN = 128


def rms_scaled(full_rows, gain_vec):
    values = full_rows.astype(jnp.float32)
    inverse = lax.rsqrt(jnp.mean(values * values, axis=-1, keepdims=True) + 1e-06)
    return (values * inverse * gain_vec).astype(jnp.bfloat16)


def add_rows(left, w_piece):
    return jnp.dot(left, w_piece, preferred_element_type=jnp.float32)


def causal_taps(product, conv_taps):
    padded = jnp.pad(product, ((0, 0), (conv_taps.shape[0] - 1, 0), (0, 0)))
    length = product.shape[1]
    summed = jnp.zeros(product.shape, jnp.float32)
    for tap_index in range(conv_taps.shape[0]):
        summed = summed + conv_taps[tap_index] * padded[:, tap_index : tap_index + length, :]
    return summed


DEPTH, WIDTH, TP = 4, 2, 4
ROWS = 256
PIECE = 512
UP, DOWN = 0, 1
SCALES, MIXER, MIXOUT, LEAD, REST, BACK, BACK_END = range(7)
MESH = pl.DeviceIdType.MESH


def block_kernel(
    tokens, g_mixer, g_ffn, w_outer, w_inner, w_value, g_outer, g_inner, g_value, g_taps,
    w_mixout, g_mixout, w_gate, w_upward, g_gate, g_upward, w_down, g_down,
    out,
    h_scales, h_mixer, h_mixout, h_lead, h_rest, h_back, h_back_end, s_lead, s_rest, raw_gate, raw_up, raw_down,
    raw_mixer, raw_mixout, raw_scale,
    mixer_gain, ffn_gain, s_outer, s_inner, s_value, taps, s_mixout, s_gate, s_upward, s_down,
    act, mixer, mixout, lead, rest, back, scales, mixed, hidden, residual_own,
    part, from_core, from_y, from_x,
    z_send, y_send, fs_recv, tp_send, tp_recv, mx_send, mx_recv, mx_whole,
    act_send, act_recv, core_send, core_recv, sum_send, sum_recv, last_send, last_recv,
    local_sem, small_sem,
):
    f32, bf16 = jnp.float32, jnp.bfloat16
    me, tp = lax.axis_index("fs"), lax.axis_index("tp")
    zed, why = lax.div(me, WIDTH), lax.rem(me, WIDTH)
    ex, core = lax.div(tp, 2), lax.rem(tp, 2)
    other = 1 - why
    last_z = DEPTH - 1
    count = tokens.shape[0]
    tiles = count // ROWS

    beside = zed * WIDTH + other
    sibling = ex * 2 + (1 - core)
    across = (1 - ex) * 2 + core

    wide = w_outer.shape[1]
    fetched = (
        (w_outer, raw_mixer.at[0]), (w_inner, raw_mixer.at[1]), (w_value, raw_mixer.at[2]),
        (w_mixout, raw_mixout), (w_gate, raw_gate), (w_upward, raw_up), (w_down, raw_down),
    )

    def fetch(k):
        return pltpu.make_async_copy(*fetched[k], local_sem.at[8 + k])

    small = (
        (g_mixout, s_mixout), (g_down, s_down), (g_gate, s_gate), (g_upward, s_upward),
        (g_mixer, mixer_gain), (g_ffn, ffn_gain), (g_outer, s_outer), (g_inner, s_inner),
        (g_value, s_value), (g_taps, taps),
    )

    def fetch_small(k):
        return pltpu.make_async_copy(*small[k], small_sem.at[k])

    for k in range(4):
        fetch(k).start()
    for k in range(len(small)):
        fetch_small(k).start()
    for k in range(4, len(fetched)):
        fetch(k).start()
    barrier = pltpu.get_barrier_semaphore()
    ring = [lax.rem(zed + step, DEPTH) * WIDTH + why for step in (1, DEPTH - 1)]
    for peer in (beside, *ring):
        pl.semaphore_signal(barrier, inc=1, device_id={"fs": peer}, device_id_type=MESH)
    for peer in (sibling, across):
        pl.semaphore_signal(barrier, inc=1, device_id={"tp": peer}, device_id_type=MESH)
    for k in range(4):
        fetch(k).wait()
    for k in range(3):
        h_mixer[:, k * wide : (k + 1) * wide] = raw_mixer[k].astype(bf16)
    h_mixout[...] = raw_mixout[...].astype(bf16)
    for k in range(2):
        fetch_small(k).wait()
    for k, row in enumerate((s_mixout, s_down)):
        h_scales[k * 4 : (k + 1) * 4, :] = jnp.broadcast_to(row[...], (4, row.shape[1]))
    pl.semaphore_wait(barrier, 5)

    fulls = (scales, mixer, mixout, lead, rest, back, back)
    split = (h_lead, h_rest, h_back, h_back_end)
    own_src = (h_scales, h_mixer, h_mixout, *[h.at[why] for h in split])

    def place(p, owner):
        if p in (MIXER, LEAD, REST):
            height = own_src[p].shape[0]
            return fulls[p].at[pl.ds(pl.multiple_of(owner * height, height), height), :]
        height, wide = own_src[p].shape
        first = pl.multiple_of(tp * height, height) if p == MIXOUT else 0
        start = owner * wide
        if p >= BACK:
            start = owner * 2 * wide + (p - BACK) * wide
        return fulls[p].at[pl.ds(first, height), pl.ds(pl.multiple_of(start, wide), wide)]

    first_own = LEAD * DEPTH - LEAD

    def kind(p, owner):
        return p if p < LEAD else LEAD + (p - LEAD) * WIDTH + lax.rem(owner, WIDTH)

    def line_of(owner, way):
        z = lax.div(owner, WIDTH)
        return z if way == UP else lax.select(z == zed, DEPTH, z)

    def z_copy(p, owner, way, src=None):
        spot = place(p, owner)
        step = 1 if way == UP else -1
        return pltpu.make_async_remote_copy(
            src_ref=spot if src is None else src,
            dst_ref=spot,
            send_sem=z_send.at[kind(p, owner), line_of(owner, way)],
            recv_sem=fs_recv.at[p, owner],
            device_id={"fs": (zed + step) * WIDTH + why},
            device_id_type=MESH,
        )

    def y_copy(p, owner, src=None):
        spot = place(p, owner)
        return pltpu.make_async_remote_copy(
            src_ref=spot if src is None else src,
            dst_ref=spot,
            send_sem=y_send.at[p * DEPTH + lax.div(owner, WIDTH) if p < LEAD else first_own + p],
            recv_sem=fs_recv.at[p, owner],
            device_id={"fs": beside},
            device_id_type=MESH,
        )

    def arrived(p, owner):
        y_copy(p, owner).wait_recv()

    def own(p):
        return pltpu.make_async_copy(own_src[p], place(p, me), local_sem.at[p])

    can_up, can_down = zed < last_z, zed > 0
    outer = (zed == 0) | (zed == last_z)

    def z_own(p, row, src):
        owner = zed * WIDTH + row
        pl.when(can_up)(lambda: z_copy(p, owner, UP, src).start())
        pl.when(can_down)(lambda: z_copy(p, owner, DOWN, src).start())

    def relay(p, s, row):
        low, high = (zed - s) * WIDTH + row, (zed + s) * WIDTH + row

        @pl.when((zed >= s) & can_up)
        def _():
            arrived(p, low)
            z_copy(p, low, UP).start()

        @pl.when((zed + s <= last_z) & can_down)
        def _():
            arrived(p, high)
            z_copy(p, high, DOWN).start()

    def settle(p, s, row):
        low, high = (zed - s) * WIDTH + row, (zed + s) * WIDTH + row
        pl.when((zed >= s) & (zed == last_z))(lambda: arrived(p, low))
        pl.when((zed + s <= last_z) & (zed == 0))(lambda: arrived(p, high))

    def mx_copy(owner, k, src=None):
        line, target = ((tp, sibling), (tp, across), (across, sibling))[k]
        height, wide = h_mixout.shape
        columns = slice(None)
        if owner is not None:
            columns = pl.ds(pl.multiple_of(owner * wide, wide), wide)
        spot = mixout.at[pl.ds(pl.multiple_of(line * height, height), height), columns]
        return pltpu.make_async_remote_copy(
            src_ref=spot if src is None else src,
            dst_ref=spot,
            send_sem=mx_send.at[k],
            recv_sem=mx_recv.at[0 if owner is None else owner] if k == 1 else mx_whole.at[k // 2],
            device_id={"tp": target},
            device_id_type=MESH,
        )

    def mx_first(owner, src=None):
        mx_copy(owner, 1, src).start()
        mx_copy(owner, 0, src).start()

    firsts = (SCALES, MIXOUT, MIXER)

    def relay_first(s):
        low, high = (zed - s) * WIDTH + why, (zed + s) * WIDTH + why

        @pl.when(zed >= s)
        def _():
            for p in firsts:
                arrived(p, low)
                pl.when(can_up)(lambda: z_copy(p, low, UP).start())
                y_copy(p, low).start()
                if p == MIXOUT:
                    mx_first(low)

        @pl.when(zed + s <= last_z)
        def _():
            for p in firsts:
                arrived(p, high)
                pl.when(can_down)(lambda: z_copy(p, high, DOWN).start())
                y_copy(p, high).start()
                if p == MIXOUT:
                    mx_first(high)

    def from_beside(s):
        def take(owner):
            for p in firsts:
                arrived(p, owner)
                if p == MIXOUT:
                    mx_first(owner)

        if s == 0:
            take(beside)
            return
        low, high = (zed - s) * WIDTH + other, (zed + s) * WIDTH + other
        pl.when(zed >= s)(lambda: take(low))
        pl.when(zed + s <= last_z)(lambda: take(high))

    base = pl.multiple_of(why * count, count)

    def tp_slot(a, owner):
        if a == 0:
            wide = tokens.shape[1]
            return act.at[pl.ds(base, count), pl.ds(pl.multiple_of(owner * wide, wide), wide)]
        wide = mixed.shape[1] // TP
        return mixed.at[:, pl.ds(pl.multiple_of(owner * wide, wide), wide)]

    def tp_copy(a, k):
        owner, target = ((tp, sibling), (tp, across), (across, sibling))[k]
        spot = tp_slot(a, owner)
        return pltpu.make_async_remote_copy(
            src_ref=tokens if a == 0 and k < 2 else spot,
            dst_ref=spot,
            send_sem=tp_send.at[a, k],
            recv_sem=tp_recv.at[a, k],
            device_id={"tp": target},
            device_id_type=MESH,
        )

    def tp_first(a):
        tp_copy(a, 1).start()
        tp_copy(a, 0).start()

    def tp_second(a):
        tp_copy(a, 1).wait_recv()
        tp_copy(a, 2).start()

    def tp_finish(a):
        tp_copy(a, 0).wait_recv()
        tp_copy(a, 2).wait_recv()

    own_tokens = pltpu.make_async_copy(tokens, tp_slot(0, tp), local_sem.at[7])

    for p in firsts:
        y_copy(p, me, own_src[p]).start()
        z_own(p, why, own_src[p])
    tp_first(0)
    mx_first(me, h_mixout)
    own_tokens.start()
    for p in firsts:
        own(p).start()
    units = h_back.shape[1]
    main = units // 128 * 128
    middle, after = pl.ds(main, 128), main + 128

    cut = h_lead.shape[2] // 2

    def share_out(gate, up, write):
        tail = main - cut
        for half, first in enumerate((0, after)):
            for k, source in enumerate((gate, up)):
                write(0, half, pl.ds(k * cut, cut), source[:, pl.ds(first, cut)])
                at = pl.ds(k * (tail + 128), tail)
                write(1, half, at, source[:, pl.ds(first + cut, tail)])
        gate, up = gate[:, middle], up[:, middle]
        low = lax.broadcasted_iota(jnp.int32, gate.shape, 1) < 64
        write(1, 0, pl.ds(tail, 128), jnp.where(low, gate, pltpu.roll(up, 64, 1)))
        write(1, 1, pl.ds(tail, 128), jnp.where(low, pltpu.roll(gate, 64, 1), up))

    def write_scale(target, half, lanes, values):
        (s_lead, s_rest)[target][half : half + 1, lanes] = values[0:1]

    def write_gated(target, half, lanes, values):
        split[target][half, :, lanes] = values.astype(bf16)

    for k in range(4, len(fetched)):
        fetch(k).wait()
    for k in range(2, len(small)):
        fetch_small(k).wait()
    share_out(raw_gate, raw_up, write_gated)
    narrow = h_back.shape[2]
    for k, target in enumerate((h_back, h_back_end)):
        lanes = pl.ds(k * narrow, narrow)
        target[0] = raw_down[:units, lanes].astype(bf16)
        target[1, :main, :] = raw_down[after:, lanes].astype(bf16)
        target[1, main:, :] = raw_down[units:after, lanes].astype(bf16)
    for k, row in enumerate((s_gate, s_upward)):
        raw_scale[k] = jnp.broadcast_to(row[...], raw_scale.shape[1:])
    share_out(raw_scale.at[0], raw_scale.at[1], write_scale)
    for p in (LEAD, REST, BACK, BACK_END):
        own(p).start()
    back[units:, :] = jnp.zeros((back.shape[0] - units, back.shape[1]), bf16)

    @pl.when(outer)
    def _():
        for p in (LEAD, REST):
            z_own(p, why, own_src[p])

    relay_first(1)
    tp_second(0)
    relay_first(2)
    pl.when(jnp.logical_not(outer))(lambda: z_own(LEAD, why, own_src[LEAD]))
    relay_first(3)
    y_copy(LEAD, me, h_lead.at[other]).start()
    y_copy(REST, me, h_rest.at[other]).start()
    relay(LEAD, 1, why)
    for s in range(DEPTH):
        from_beside(s)
    relay(LEAD, 2, why)
    tp_finish(0)
    own_tokens.wait()
    for p in firsts:
        own(p).wait()

    chan = mixed.shape[1] // TP

    def tile(i):
        return pl.ds(pl.multiple_of(i * ROWS, ROWS), ROWS)

    def own_rows(i):
        return pl.ds(pl.multiple_of(base + i * ROWS, ROWS), ROWS)

    def normalised(values, gain):
        inverse = lax.rsqrt(jnp.mean(values * values, axis=-1, keepdims=True) + 1e-06)
        return (values * inverse * gain[...]).astype(bf16)

    @pl.loop(0, tiles)
    def _(i):
        normed = normalised(act[own_rows(i), :].astype(f32), mixer_gain)
        three = jnp.dot(normed, mixer[...], preferred_element_type=f32)
        product = (three[:, chan : 2 * chan] * s_inner[...]) * (three[:, 2 * chan :] * s_value[...])
        row = lax.rem(lax.broadcasted_iota(jnp.int32, product.shape, 0), SEQ_LEN)
        total = jnp.zeros_like(product)
        last = taps.shape[0] - 1
        for j in range(taps.shape[0]):
            gap = last - j
            moved = product
            if gap:
                moved = jnp.where(row >= gap, pltpu.roll(product, gap, 0), 0.0)
            total = total + taps[j : j + 1, :] * moved
        mixed[tile(i), pl.ds(pl.multiple_of(tp * chan, chan), chan)] = (
            three[:, :chan] * s_outer[...] * total
        ).astype(bf16)

    tp_first(1)
    arrived(LEAD, beside)
    z_own(LEAD, other, None)
    pl.when(jnp.logical_not(outer))(lambda: z_own(REST, why, own_src[REST]))
    for owner in range(DEPTH * WIDTH):
        mx_copy(owner, 1).wait_recv()
        mx_copy(owner, 2).start()
    tp_second(1)
    relay(LEAD, 1, other)
    mx_copy(None, 0).wait_recv()
    mx_copy(None, 2).wait_recv()
    tp_finish(1)
    for k in range(3):
        tp_copy(0, k).wait_send()

    arrived(REST, beside)
    z_own(REST, other, None)

    feat = tokens.shape[1]
    quarter = count // TP
    strip = quarter // 2

    def act_copy(k, h):
        half, owner, target = (
            (why, tp, {"fs": beside}),
            (other, tp, {"tp": sibling}),
            (other, tp, {"tp": across}),
            (other, across, {"tp": sibling}),
        )[k]
        first = half * count + owner * quarter + h * strip
        spot = act.at[pl.ds(pl.multiple_of(first, strip), strip), :]
        return pltpu.make_async_remote_copy(
            src_ref=spot,
            dst_ref=spot,
            send_sem=act_send.at[k, h],
            recv_sem=act_recv.at[k, h],
            device_id=target,
            device_id_type=MESH,
        )

    @pl.loop(0, tiles)
    def _(step):
        i = lax.rem(step + tp, tiles)
        term = jnp.dot(mixed[tile(i), :], mixout[...], preferred_element_type=f32)
        term = term * scales[0:1, :]
        residual = (act[own_rows(i), :].astype(f32) + term).astype(bf16)
        act[own_rows(i), :] = residual
        residual_own[tile(i), :] = act[
            own_rows(i), pl.ds(pl.multiple_of(tp * feat, feat), feat)
        ]
        act[own_rows(i), :] = normalised(residual.astype(f32), ffn_gain)

        @pl.when(step == 0)
        def _():
            for h in range(2):
                act_copy(0, h).start()

    y_copy(BACK, me, h_back.at[other]).start()
    y_copy(BACK_END, me, h_back_end.at[other]).start()

    def spread_act(h):
        act_copy(0, h).wait_recv()
        act_copy(2, h).start()
        act_copy(1, h).start()

    spread_act(0)
    relay(LEAD, 2, other)
    relay(REST, 1, why)
    spread_act(1)
    relay(REST, 2, why)
    relay(REST, 1, other)

    def sent(p, row):
        owner = zed * WIDTH + row
        pl.when(can_up)(lambda: z_copy(p, owner, UP).wait_send())
        pl.when(can_down)(lambda: z_copy(p, owner, DOWN).wait_send())
        for s in (1, 2):
            low, high = (zed - s) * WIDTH + row, (zed + s) * WIDTH + row
            pl.when((zed >= s) & can_up)(lambda: z_copy(p, low, UP).wait_send())
            pl.when((zed + s <= last_z) & can_down)(lambda: z_copy(p, high, DOWN).wait_send())

    for p in firsts:
        sent(p, why)
        y_copy(p, me).wait_send()
        for s in (1, 2, 3):
            low, high = (zed - s) * WIDTH + why, (zed + s) * WIDTH + why
            pl.when(zed >= s)(lambda: y_copy(p, low).wait_send())
            pl.when(zed + s <= last_z)(lambda: y_copy(p, high).wait_send())
    for k in range(3):
        mx_copy(None, k).wait_send()
    for k in range(3):
        tp_copy(1, k).wait_send()

    for h in range(2):
        act_copy(2, h).wait_recv()
        act_copy(3, h).start()
    relay(REST, 2, other)
    for p in (BACK, BACK_END):
        arrived(p, beside)
        own(p).wait()
    for row in range(WIDTH):
        for p in (BACK, BACK_END):
            z_own(p, row, None)
    for p in (LEAD, REST):
        own(p).wait()
    for row in (why, other):
        for s in (1, 2, 3):
            settle(LEAD, s, row)
    for h in range(2):
        act_copy(1, h).wait_recv()
        act_copy(3, h).wait_recv()

    def activate(weights, row_scales, first, write):
        @pl.loop(0, tiles)
        def _(i):
            rows = pl.ds(pl.multiple_of(first + i * ROWS, ROWS), ROWS)
            both = jnp.dot(act[rows, :], weights[...], preferred_element_type=f32)
            write(rows, both * row_scales[pl.ds(why, 1), :])

    def gate_with(gate, up):
        return gate / (1.0 + jnp.exp(-gate)) * up

    def write_lead(rows, both):
        hidden[rows, :cut] = gate_with(both[:, :cut], both[:, cut:]).astype(bf16)

    def write_rest(rows, both):
        tail = main - cut
        hidden[rows, cut:main] = gate_with(both[:, :tail], both[:, tail + 128 :]).astype(bf16)
        mixed_lanes = both[:, tail : tail + 128]
        ends = gate_with(mixed_lanes, pltpu.roll(mixed_lanes, 64, 1))
        lane = lax.broadcasted_iota(jnp.int32, ends.shape, 1)
        hidden[rows, main:] = jnp.where(lane < 64, ends, 0.0).astype(bf16)

    for half in (other, why):
        activate(lead, s_lead, half * count, write_lead)
    for row in (why, other):
        for s in (1, 2, 3):
            settle(REST, s, row)

    pieces = count // PIECE

    def piece(t):
        return pl.ds(pl.multiple_of(t * PIECE, PIECE), PIECE)

    def block_at(k):
        return lax.rem(zed + k * (1 - 2 * lax.div(zed, last_z)) + DEPTH, DEPTH)

    def region(ref, half, q, by_columns):
        if by_columns:
            wide = h_back.shape[2]
            return ref.at[pl.ds(pl.multiple_of(half * count, count), count), pl.ds(q * wide, wide)]
        return ref.at[piece(half * pieces + q), :]

    def core_copy(j, row, half, q, by_columns):
        line, t = lax.div(j, 2), half * pieces + q
        return pltpu.make_async_remote_copy(
            src_ref=region(part.at[j, row], half, q, by_columns),
            dst_ref=region(from_core.at[line, row], half, q, by_columns),
            send_sem=core_send.at[line, row],
            recv_sem=core_recv.at[line, row, t],
            device_id={"tp": sibling},
            device_id_type=MESH,
        )

    def sum_copy(j, row, q, by_columns):
        line = lax.div(j, 2)
        return pltpu.make_async_remote_copy(
            src_ref=region(part.at[j, row], other, q, by_columns),
            dst_ref=region(from_y.at[line, row], 0, q, by_columns),
            send_sem=sum_send.at[line, row, q],
            recv_sem=sum_recv.at[line, row, q],
            device_id={"fs": beside},
            device_id_type=MESH,
        )

    def last_copy(j, row, q, by_columns):
        return pltpu.make_async_remote_copy(
            src_ref=region(part.at[j, row], why, q, by_columns),
            dst_ref=region(from_x.at[row], 0, q, by_columns),
            send_sem=last_send.at[row, q],
            recv_sem=last_recv.at[row, q],
            device_id={"tp": across},
            device_id_type=MESH,
        )

    def is_last(k, row):
        return k == last_z and row == WIDTH - 1

    def multiply(k, row, half):
        j = block_at(k)
        wide = 2 * h_back.shape[2]
        columns = pl.ds(pl.multiple_of((j * WIDTH + row) * wide, wide), wide)

        @pl.loop(0, pieces)
        def _(q):
            t = half * pieces + q
            term = jnp.dot(hidden[piece(t), :], back[:, columns], preferred_element_type=f32)
            part[j, row, piece(t), :] = (term * scales[4:5, columns]).astype(bf16)
            pl.when(core != lax.rem(j, 2))(lambda: core_copy(j, row, half, q, False).start())

    def multiply_narrow(k, row, half, q):
        j = block_at(k)
        wide = h_back.shape[2]
        start = (j * WIDTH + row) * 2 * wide + q * wide
        columns = pl.ds(pl.multiple_of(start, wide), wide)

        @pl.loop(0, pieces)
        def _(i):
            t = half * pieces + i
            term = jnp.dot(hidden[piece(t), :], back[:, columns], preferred_element_type=f32)
            part[j, row, piece(t), pl.ds(q * wide, wide)] = (
                term * scales[4:5, columns]
            ).astype(bf16)

        pl.when(core != lax.rem(j, 2))(lambda: core_copy(j, row, half, q, True).start())

    def added(j, row, half, q, by_columns, extra):
        spot = region(part.at[j, row], half, q, by_columns)
        return spot[...].astype(f32) + extra[...].astype(f32)

    def stage_1(k, row, half, some=None):
        j, by = block_at(k), is_last(k, row)

        @pl.when(core == lax.rem(j, 2))
        def _():
            line = lax.div(j, 2)
            for q in range(pieces) if some is None else (some,):
                core_copy(j, row, half, q, by).wait_recv()
                extra = region(from_core.at[line, row], half, q, by)
                total = added(j, row, half, q, by, extra)
                region(part.at[j, row], half, q, by)[...] = total.astype(bf16)
                if half is other:
                    sum_copy(j, row, q, by).start()

    def stage_2(k, row, some=None):
        j, by = block_at(k), is_last(k, row)

        @pl.when(core == lax.rem(j, 2))
        def _():
            line = lax.div(j, 2)
            for q in range(pieces) if some is None else (some,):
                sum_copy(j, row, q, by).wait_recv()
                total = added(j, row, why, q, by, region(from_y.at[line, row], 0, q, by))
                region(part.at[j, row], why, q, by)[...] = total.astype(bf16)
                pl.when(ex != line)(lambda: last_copy(j, row, q, by).start())

    def stage_3(k, row):
        j, by = block_at(k), is_last(k, row)
        wide = 2 * h_back.shape[2]

        @pl.when(tp == j)
        def _():
            for q in range(pieces):
                last_copy(j, row, q, by).wait_recv()
                total = added(j, row, why, q, by, region(from_x.at[row], 0, q, by))
                lanes = pl.ds(row * wide, wide)
                kept = region(residual_own.at[:, lanes], 0, q, by)[...].astype(f32)
                region(out.at[:, lanes], 0, q, by)[...] = (kept + total).astype(bf16)

    activate(rest, s_rest, other * count, write_rest)
    for row in range(WIDTH):
        for p in (BACK, BACK_END):
            relay(p, 1, row)
    for row in range(WIDTH):
        multiply(0, row, other)
        stage_1(0, row, other)
    activate(rest, s_rest, base, write_rest)
    for row in range(WIDTH):
        multiply(0, row, why)
        stage_1(0, row, why)

    order = [(k, row) for k in range(DEPTH) for row in range(WIDTH)]
    after_unit = {
        3: ((stage_2, 0), (stage_2, 1)),
        4: ((stage_2, 2),),
        5: ((stage_2, 3), (stage_2, 4)),
        6: ((stage_2, 5), (stage_3, 0), (stage_3, 1)),
        7: (
            (stage_2, 7), (stage_3, 2), (stage_3, 3), (stage_3, 4), (stage_3, 5),
            (stage_3, 6), (stage_3, 7),
        ),
    }
    for u, (k, row) in enumerate(order):
        if u == 2 * WIDTH:
            for line in range(WIDTH):
                for p in (BACK, BACK_END):
                    relay(p, 2, line)
        if k:
            owner = block_at(k) * WIDTH + row
            if is_last(k, row):
                for q in range(pieces):
                    pl.when(outer)(lambda: arrived(BACK + q, owner))
                    for half in (other, why):
                        multiply_narrow(k, row, half, q)
                        stage_1(k, row, half, q)
                    stage_2(*order[u - 1], q)
            else:
                for p in (BACK, BACK_END):
                    pl.when(outer)(lambda: arrived(p, owner))
                for half in (other, why):
                    multiply(k, row, half)
                    stage_1(k, row, half)
        for stage, unit in after_unit.get(u, ()):
            stage(*order[unit])

    for p in (LEAD, REST, BACK, BACK_END):
        y_copy(p, me).wait_send()
        for row in range(WIDTH):
            sent(p, row)
    for k in range(4):
        for h in range(2):
            act_copy(k, h).wait_send()
    for k, row in order:
        j = block_at(k)

        @pl.when(core != lax.rem(j, 2))
        def _():
            pltpu.make_async_remote_copy(
                src_ref=part.at[j, row],
                dst_ref=from_core.at[lax.div(j, 2), row],
                send_sem=core_send.at[lax.div(j, 2), row],
                recv_sem=core_recv.at[lax.div(j, 2), row, 0],
                device_id={"tp": sibling},
                device_id_type=MESH,
            ).wait_send()

        @pl.when(core == lax.rem(j, 2))
        def _():
            for q in range(pieces):
                by = is_last(k, row)
                sum_copy(j, row, q, by).wait_send()
                pl.when(ex != lax.div(j, 2))(lambda: last_copy(j, row, q, by).wait_send())


def fused_device(
    tokens,
    mixer_gain,
    ffn_gain,
    w_outer,
    w_inner,
    w_value,
    scale_outer,
    scale_inner,
    scale_value,
    conv_taps,
    w_mixout,
    scale_mixout,
    w_gate,
    w_upward,
    scale_gate,
    scale_upward,
    w_down,
    scale_down,
):
    bf16 = jnp.bfloat16
    count, feat = tokens.shape
    model = mixer_gain.shape[0]
    chan = w_outer.shape[1]
    units = w_gate.shape[1]
    cols = w_down.shape[1]
    half = units // 2
    padded = half // 128 * 128 + 128
    cut = half // 128 * 4 // 5 * 128
    vmem = pl.BlockSpec(memory_space=pltpu.VMEM)
    hbm = pl.BlockSpec(memory_space=pl.ANY)
    dma = pltpu.SemaphoreType.DMA
    owners = DEPTH * WIDTH
    return pl.pallas_call(
        block_kernel,
        out_shape=pltpu.VMEM((count, feat), bf16),
        in_specs=[hbm] * 18,
        out_specs=vmem,
        scratch_shapes=[
            pltpu.VMEM((8, cols), jnp.float32),
            pltpu.VMEM((w_outer.shape[0], 3 * chan), bf16),
            pltpu.VMEM(w_mixout.shape, bf16),
            pltpu.VMEM((2, w_gate.shape[0], 2 * cut), bf16),
            pltpu.VMEM((2, w_gate.shape[0], units - 2 * cut), bf16),
            pltpu.VMEM((2, half, cols // 2), bf16),
            pltpu.VMEM((2, half, cols // 2), bf16),
            pltpu.VMEM((2, 2 * cut), jnp.float32),
            pltpu.VMEM((2, units - 2 * cut), jnp.float32),
            pltpu.VMEM(w_gate.shape, jnp.float32),
            pltpu.VMEM(w_upward.shape, jnp.float32),
            pltpu.VMEM(w_down.shape, jnp.float32),
            pltpu.VMEM((3, *w_outer.shape), jnp.float32),
            pltpu.VMEM(w_mixout.shape, jnp.float32),
            pltpu.VMEM((2, 8, units), jnp.float32),
            *[
                pltpu.VMEM(row, jnp.float32)
                for row in (
                    (1, model), (1, model), scale_outer.shape, scale_inner.shape,
                    scale_value.shape, conv_taps.shape, scale_mixout.shape, scale_gate.shape,
                    scale_upward.shape, scale_down.shape,
                )
            ],
            pltpu.VMEM((WIDTH * count, model), bf16),
            pltpu.VMEM((model, 3 * chan), bf16),
            pltpu.VMEM((TP * chan, model), bf16),
            pltpu.VMEM((model, 2 * cut), bf16),
            pltpu.VMEM((model, units - 2 * cut), bf16),
            pltpu.VMEM((padded, model), bf16),
            pltpu.VMEM((8, model), jnp.float32),
            pltpu.VMEM((count, TP * chan), bf16),
            pltpu.VMEM((WIDTH * count, padded), bf16),
            pltpu.VMEM((count, feat), bf16),
            pltpu.VMEM((DEPTH, WIDTH, WIDTH * count, cols), bf16),
            pltpu.VMEM((2, WIDTH, WIDTH * count, cols), bf16),
            pltpu.VMEM((2, WIDTH, count, cols), bf16),
            pltpu.VMEM((WIDTH, count, cols), bf16),
            dma((11, DEPTH + 1)),
            dma((3 * DEPTH + 4,)),
            dma((7, owners)),
            dma((2, 3)),
            dma((2, 3)),
            dma((3,)),
            dma((owners,)),
            dma((2,)),
            dma((4, 2)),
            dma((4, 2)),
            dma((2, WIDTH)),
            dma((2, WIDTH, 4)),
            dma((2, WIDTH, 2)),
            dma((2, WIDTH, 2)),
            dma((WIDTH, 2)),
            dma((WIDTH, 2)),
            dma((15,)),
            dma((10,)),
        ],
        compiler_params=pltpu.CompilerParams(
            collective_id=0, has_side_effects=True, vmem_limit_bytes=62 * 1024 * 1024
        ),
    )(
        tokens, mixer_gain[None], ffn_gain[None], w_outer, w_inner, w_value,
        scale_outer, scale_inner, scale_value, conv_taps, w_mixout, scale_mixout,
        w_gate, w_upward, scale_gate, scale_upward, w_down, scale_down,
    )


def plain_device(
    tokens,
    mixer_gain,
    ffn_gain,
    w_outer,
    w_inner,
    w_value,
    scale_outer,
    scale_inner,
    scale_value,
    conv_taps,
    w_mixout,
    scale_mixout,
    w_gate,
    w_upward,
    scale_gate,
    scale_upward,
    w_down,
    scale_down,
):
    full_rows = lax.all_gather(tokens, "tp", axis=1, tiled=True)
    normed = rms_scaled(full_rows, mixer_gain)
    tok_count = tokens.shape[0]
    local_channels = w_outer.shape[1]

    def add_one(w_piece):
        return add_rows(normed, w_piece)

    outer_bf = w_outer.astype(jnp.bfloat16)
    inner_bf = w_inner.astype(jnp.bfloat16)
    value_bf = w_value.astype(jnp.bfloat16)
    outer = add_one(lax.all_gather(outer_bf, "fs", axis=0, tiled=True))
    inner = add_one(lax.all_gather(inner_bf, "fs", axis=0, tiled=True))
    value = add_one(lax.all_gather(value_bf, "fs", axis=0, tiled=True))
    outer = outer * scale_outer
    product = inner * scale_inner * (value * scale_value)
    product = product.reshape(tok_count // SEQ_LEN, SEQ_LEN, local_channels)
    conv = causal_taps(product, conv_taps).reshape(tok_count, local_channels)
    mixed_out = (outer * conv).astype(jnp.bfloat16)
    mixout_scales, down_scales = (
        lax.all_gather(scale_mixout, "fs", axis=1, tiled=True),
        lax.all_gather(scale_down, "fs", axis=1, tiled=True),
    )
    mixout_bf = w_mixout.astype(jnp.bfloat16)
    mixed_all = lax.all_gather(mixed_out, "tp", axis=1, tiled=True)
    mixout_cols = lax.all_gather(mixout_bf, "fs", axis=1, tiled=True)
    mixout_all = lax.all_gather(mixout_cols, "tp", axis=0, tiled=True)
    mix_term = jnp.dot(mixed_all, mixout_all, preferred_element_type=jnp.float32) * mixout_scales
    residual_rows = (full_rows.astype(jnp.float32) + mix_term).astype(jnp.bfloat16)
    feature_count = tokens.shape[1]
    residual = lax.dynamic_slice_in_dim(
        residual_rows, lax.axis_index("tp") * feature_count, feature_count, 1
    )
    normed_ffn = rms_scaled(residual_rows, ffn_gain)
    gate_proj = add_rows(
        normed_ffn, lax.all_gather(w_gate.astype(jnp.bfloat16), "fs", axis=0, tiled=True)
    )
    up_proj = add_rows(
        normed_ffn, lax.all_gather(w_upward.astype(jnp.bfloat16), "fs", axis=0, tiled=True)
    )
    hidden = (jax.nn.silu(gate_proj * scale_gate) * (up_proj * scale_upward)).astype(jnp.bfloat16)
    down_terms = (
        jnp.dot(
            hidden,
            lax.all_gather(w_down.astype(jnp.bfloat16), "fs", axis=1, tiled=True),
            preferred_element_type=jnp.float32,
        )
        * down_scales
    )
    ffn_share = lax.psum_scatter(
        down_terms.astype(jnp.bfloat16), "tp", scatter_dimension=1, tiled=True
    ).astype(jnp.float32)
    return (residual.astype(jnp.float32) + ffn_share).astype(jnp.bfloat16)


def solution(mesh):
    in_specs = (
        P("fs", "tp"),
        P(),
        P(),
        P("fs", "tp"),
        P("fs", "tp"),
        P("fs", "tp"),
        P(None, "tp"),
        P(None, "tp"),
        P(None, "tp"),
        P(None, "tp"),
        P("tp", "fs"),
        P(None, "fs"),
        P("fs", "tp"),
        P("fs", "tp"),
        P(None, "tp"),
        P(None, "tp"),
        P("tp", "fs"),
        P(None, "fs"),
    )
    out_specs = P("fs", "tp")
    chosen = fused_device if (mesh.shape["fs"], mesh.shape["tp"]) == (8, 4) else plain_device
    return jax.shard_map(
        chosen, mesh=mesh, in_specs=in_specs, out_specs=out_specs, check_vma=False
    )
```
